512 devices in a mesh: sp: 64 (over z, y), tp: 8 (over x, core).
Axes of the slice: x: 4, y: 4, z: 16, core: 2. Of those that a mesh axis runs over, the one named last changes fastest.
Arguments:
- tokens: bfloat16 [24576, 2048], P(('sp', 'tp')), may hold values from -6 to 6
- query_weight: bfloat16 [2048, 1024], P(None, 'tp'), may hold values from -0.125 to 0.125
- key_weight: bfloat16 [2048, 1024], P(None, 'tp'), may hold values from -0.125 to 0.125
- value_weight: bfloat16 [2048, 1024], P(None, 'tp'), may hold values from -0.125 to 0.125
- query_gain: float32 [64], replicated, may hold values from 0.5 to 16
- key_gain: float32 [64], replicated, may hold values from 0.5 to 16
- log_gate_total: float32 [24576, 16], P('sp', 'tp'), may hold values from -3510 to 0, as said below
- output_weight: bfloat16 [1024, 2048], P('tp'), may hold values from -0.1875 to 0.1875
Outputs:
- mixed: bfloat16 [24576, 2048], P(('sp', 'tp'))
The draws below stay inside these ranges and needn't reach their ends.
Inputs may be any that keep to these rules, and one draw needn't show every extreme that they name: `log_gate_total`: each column never rises from one position to the next.
All inputs are finite; a program needn't handle non-finite values.
Results may differ from the reference program's by a relative error of at most 0.014.
The reference program's roundings to bfloat16 on the way count: a program that leaves them out, or rounds other values in their place, can miss the bound.
Values may be sent and summed in bfloat16 or wider, within the bound.
A program may use at most 64 MiB of HBM per device.

```python
import math
import jax
import jax.numpy as jnp
from jax import lax

D = 2048
HEADS = 16
HEAD_SIZE = 64
TOK_DEV = 384
TOKENS = 24576
N_TP = 8


def gain_draw(key, salt_number):
    values = jax.random.uniform(jax.random.fold_in(key, salt_number), (HEAD_SIZE,), jnp.float32, 0.5, 1.5)
    return values


def draw_query_gain(key, part):
    return gain_draw(key, 21)


def draw_key_gain(key, part):
    return gain_draw(key, 22)


def draw_log_gate_total(key, part):
    head_order = jax.random.permutation(jax.random.fold_in(key, 31), HEADS)
    slow_count = HEADS // 2
    is_slow = head_order < slow_count
    slow_rate = jax.random.uniform(jax.random.fold_in(key, 32), (HEADS,), jnp.float32, 0.3, 1.5) / TOKENS
    fast_rate = 1.0 / jax.random.uniform(jax.random.fold_in(key, 33), (HEADS,), jnp.float32, 30.0, 100.0)
    base_rate = jnp.where(is_slow, slow_rate, fast_rate)
    block_factor = jnp.exp(jax.random.uniform(jax.random.fold_in(key, 34), (TOKENS // TOK_DEV, HEADS), jnp.float32, -0.8, 0.8))
    block_factor = jnp.repeat(block_factor, TOK_DEV, axis=0)
    jitter = jax.random.uniform(jax.random.fold_in(key, 35), (TOKENS, HEADS), jnp.float32, 0.2, 1.8)
    steps_down = -base_rate[None, :] * block_factor * jitter
    return jnp.cumsum(steps_down, axis=0)


def levels(key, dims, cuts, least, top_value):
    def one(dim, parts):
        heights = jax.random.uniform(jax.random.fold_in(jax.random.fold_in(key, 6), dim), (parts,), jnp.float32, least / len(cuts), top_value / len(cuts))
        return jnp.repeat(jnp.exp(heights), dims[dim] // parts).reshape((-1,) + (1,) * (len(dims) - dim - 1))

    factor_of = one(*cuts[0])
    for cut in cuts[1:]:
        factor_of = factor_of * one(*cut)
    return factor_of


def normal_values(own_key, extent, deviation, most, cuts=(), kind=jnp.bfloat16):
    drawn = jax.random.normal(own_key, extent, jnp.float32) * deviation
    if len(cuts) > 0:
        drawn = levels(own_key, extent, cuts, -0.22, 0.18) * drawn
    return jnp.clip(drawn, min=-most, max=most).astype(kind)


def setup_inputs(seed: int = 0) -> dict:
    key_of = jax.random.split(jax.random.key(seed), 9)
    return {
        "tokens": normal_values(key_of[0], (TOKENS, D), 1.0, 6.0, ((0, 512),)),
        "query_weight": normal_values(key_of[1], (D, HEADS * HEAD_SIZE), D ** -0.5, 0.125, ((1, 8),)),
        "key_weight": normal_values(key_of[2], (D, HEADS * HEAD_SIZE), D ** -0.5, 0.125, ((1, 8),)),
        "value_weight": normal_values(key_of[3], (D, HEADS * HEAD_SIZE), D ** -0.5, 0.125, ((1, 8),)),
        "query_gain": draw_query_gain(jax.random.fold_in(key_of[8], 71), 0),
        "key_gain": draw_key_gain(jax.random.fold_in(key_of[8], 71), 0),
        "log_gate_total": draw_log_gate_total(jax.random.fold_in(key_of[8], 71), 0),
        "output_weight": normal_values(key_of[7], (HEADS * HEAD_SIZE, D), (HEADS * HEAD_SIZE) ** -0.5, 0.1875, ((0, 8),)),
    }


NORM_EPS = 1e-06

def head_norm(raw, gain, head_count):
    row_count = raw.shape[0]
    split = raw.reshape(row_count, head_count, -1)
    scaled = split * lax.rsqrt(lax.optimization_barrier(jnp.mean(split * split, axis=-1, keepdims=True)) + NORM_EPS) * gain.astype(jnp.float32)
    return scaled.reshape(row_count, -1).astype(jnp.bfloat16)

def reference(tokens, query_weight, key_weight, value_weight, query_gain, key_gain, log_gate_total, output_weight):
    queries = head_norm(jnp.dot(tokens, query_weight, preferred_element_type=jnp.float32), query_gain, HEADS)
    keys = head_norm(jnp.dot(tokens, key_weight, preferred_element_type=jnp.float32), key_gain, HEADS)
    values = jnp.dot(tokens, value_weight, preferred_element_type=jnp.float32).astype(jnp.bfloat16)
    seq_len = tokens.shape[0]
    block_rows = math.gcd(seq_len, 512)
    key_pos = jnp.arange(seq_len, dtype=jnp.int32)
    score_scale = HEAD_SIZE ** (-0.5)

    def one_head(inputs):
        query_head, key_head, value_head, gate_head = inputs

        def one_block(block_index):
            first_row = (block_index * block_rows).astype(jnp.int32)
            query_block = lax.dynamic_slice_in_dim(query_head, first_row, block_rows, 0)
            gate_block = lax.dynamic_slice_in_dim(gate_head, first_row, block_rows, 0)
            scores = jnp.dot(query_block, key_head.T, preferred_element_type=jnp.float32) * score_scale
            scores = scores + gate_block[:, None] - gate_head[None, :]
            query_pos = first_row + jnp.arange(block_rows, dtype=jnp.int32)
            scores = jnp.where(query_pos[:, None] >= key_pos[None, :], scores, -jnp.inf)
            row_max = lax.optimization_barrier(jnp.max(scores, axis=1, keepdims=True))
            weights = jnp.exp(scores - row_max)
            totals = lax.optimization_barrier(jnp.sum(weights, axis=1, keepdims=True))
            summed = jnp.dot(weights.astype(jnp.bfloat16), value_head, preferred_element_type=jnp.float32)
            return (summed / totals).astype(jnp.bfloat16)
        blocks = lax.map(one_block, jnp.arange(seq_len // block_rows, dtype=jnp.int32))
        return blocks.reshape(seq_len, HEAD_SIZE)

    def by_heads(matrix):
        return matrix.reshape(seq_len, HEADS, HEAD_SIZE).transpose(1, 0, 2)
    attended = lax.map(one_head, (by_heads(queries), by_heads(keys), by_heads(values), log_gate_total.T))
    attended = attended.transpose(1, 0, 2).reshape(seq_len, HEADS * HEAD_SIZE)
    group_cols = HEADS * HEAD_SIZE // N_TP
    mixed = jnp.zeros((seq_len, D), jnp.float32)
    for part_index in range(N_TP):
        lower = part_index * group_cols
        partial_sum = jnp.dot(attended[:, lower:lower + group_cols], output_weight[lower:lower + group_cols], preferred_element_type=jnp.float32)
        rounded = lax.optimization_barrier(partial_sum.astype(jnp.bfloat16))
        mixed = mixed + rounded.astype(jnp.float32)
    return mixed.astype(jnp.bfloat16)
```

```python
import functools

import jax
import jax.numpy as jnp
from jax import lax
from jax.experimental import pallas as pl
from jax.experimental.pallas import tpu as pltpu
from jax.sharding import PartitionSpec as P

NORM_EPS = 1e-06
MESH = pl.DeviceIdType.MESH
F32 = jnp.float32
BF16 = jnp.bfloat16
LANES = 128
HEAD = 64
NX = 4
NY = 4
NC = 2
SUB = 256
QT = 256


class RowGather:
    def __init__(self, buf, rows, x, c, ids, ssem, rsem):
        self.buf, self.rows, self.x, self.c = buf, rows, x, c
        self.right, self.left, self.partner = ids
        self.ssem, self.rsem = ssem, rsem
        self.half = buf.shape[1] // 2

    def piece(self, dx, core, part):
        slot = lax.rem(self.x + dx + NX, NX) * NC + core
        rows = pl.ds(pl.multiple_of(slot * self.rows, self.rows), self.rows)
        if part is None:
            return self.buf.at[rows]
        return self.buf.at[rows, pl.ds(part * self.half, self.half)]

    def copy(self, dx, core, part, index):
        device = self.right if index < 3 else self.left if index < 6 else self.partner
        piece = self.piece(dx, core, part)
        return pltpu.make_async_remote_copy(
            src_ref=piece,
            dst_ref=piece,
            send_sem=self.ssem.at[index],
            recv_sem=self.rsem.at[index],
            device_id=device,
            device_id_type=MESH,
        )

    def send(self, dx, part, index):
        self.copy(dx, self.c, part, index).start()

    def arrive(self, dx, core, part, index):
        self.copy(dx, core, part, index).wait_recv()

    def start(self):
        self.send(0, 0, 0)
        self.send(0, 1, 3)
        self.send(0, 1, 1)
        self.send(0, 0, 4)
        self.send(0, None, 6)

    def relay(self):
        self.arrive(-1, self.c, 0, 0)
        self.send(-1, 0, 2)
        self.arrive(1, self.c, 1, 3)
        self.send(1, 1, 5)
        self.send(-1, 0, 7)
        self.send(1, 1, 8)

    def finish_links(self):
        self.arrive(-1, self.c, 1, 1)
        self.send(-1, 1, 9)
        self.arrive(1, self.c, 0, 4)
        self.send(1, 0, 10)
        self.arrive(-2, self.c, 0, 2)
        self.send(-2, 0, 11)
        self.arrive(2, self.c, 1, 5)
        self.send(2, 1, 12)

    def finish(self):
        other = 1 - self.c
        self.arrive(0, other, None, 6)
        self.arrive(-1, other, 0, 7)
        self.arrive(1, other, 1, 8)
        self.arrive(-1, other, 1, 9)
        self.arrive(1, other, 0, 10)
        self.arrive(-2, other, 0, 11)
        self.arrive(2, other, 1, 12)

    def drain(self):
        sent = [(0, 0, 0), (0, 1, 3), (0, 1, 1), (0, 0, 4), (0, None, 6), (-1, 0, 2), (1, 1, 5)]
        sent += [(-1, 0, 7), (1, 1, 8), (-1, 1, 9), (1, 0, 10), (-2, 0, 11), (2, 1, 12)]
        for dx, part, index in sent:
            self.copy(dx, self.c, part, index).wait_send()


def kernel(
    nz,
    tokens_ref,
    wq_ref,
    wk_ref,
    wv_ref,
    qgain_ref,
    kgain_ref,
    gates_ref,
    wout_ref,
    out_ref,
    tok,
    wqkv,
    wout,
    raw,
    kv_send,
    q_send,
    q_recv,
    gate_recv,
    kv_all,
    gate_all,
    q_s,
    gt_s,
    m_s,
    o_s,
    v_s,
    att_send,
    att_recv,
    lsem,
    tok_ss,
    tok_rs,
    wo_ss,
    wo_rs,
    a2a_ss,
    a2a_rs,
    ring_ss,
    ring_rs,
    d2d_ss,
    d2d_rs,
    gring_ss,
    gring_rs,
    gd2d_ss,
    gd2d_rs,
    own_ss,
    own_rs,
    att_ss,
    att_rs,
):
    sp = lax.axis_index("sp")
    tp = lax.axis_index("tp")
    z, y = lax.div(sp, NY), lax.rem(sp, NY)
    x, c = lax.div(tp, NC), lax.rem(tp, NC)

    def device(dz, dy, dx, dc):
        return (dz * NY + dy, dx * NC + dc)

    right = device(z, y, lax.rem(x + 1, NX), c)
    left = device(z, y, lax.rem(x + NX - 1, NX), c)
    partner = device(z, y, x, 1 - c)
    up = device(lax.rem(z + 1, nz), y, x, c)
    down = device(lax.rem(z + nz - 1, nz), y, x, c)
    owner_core = lax.div(y, 2)

    rows_tp = tokens_ref.shape[0]
    blk = rows_tp * NX * NC
    half = 2 * blk
    width = wq_ref.shape[1]

    own_rows = pl.ds(pl.multiple_of(tp * rows_tp, rows_tp), rows_tp)
    wout_rows = wout_ref.shape[0]
    load_tok = pltpu.make_async_copy(tokens_ref, tok.at[own_rows], lsem.at[0])
    load_tok.start()
    loads = []
    for i, w_ref in enumerate((wq_ref, wk_ref, wv_ref)):
        loads.append(
            pltpu.make_async_copy(w_ref, wqkv.at[:, pl.ds(i * width, width)], lsem.at[1 + i])
        )
    load_wout = pltpu.make_async_copy(
        wout_ref,
        wout.at[pl.ds(pl.multiple_of(tp * wout_rows, wout_rows), wout_rows)],
        lsem.at[4],
    )
    for load in loads:
        load.start()
    load_wout.start()

    barrier = pltpu.get_barrier_semaphore()
    for neighbour in (right, left, partner, up, down):
        pl.semaphore_signal(barrier, inc=1, device_id=neighbour, device_id_type=MESH)
    for i in range(2):
        j = 2 * c + i

        @pl.when(j != y)
        def _():
            pl.semaphore_signal(
                barrier, inc=1, device_id=device(z, j, x, owner_core), device_id_type=MESH
            )

    @pl.when(owner_core == c)
    def _():
        pl.semaphore_wait(barrier, 6)

    @pl.when(owner_core != c)
    def _():
        pl.semaphore_wait(barrier, 7)

    load_tok.wait()
    tok_gather = RowGather(tok, rows_tp, x, c, (right, left, partner), tok_ss, tok_rs)
    tok_gather.start()
    tok_gather.relay()
    tok_gather.finish_links()
    load_wout.wait()
    wout_gather = RowGather(wout, wout_rows, x, c, (right, left, partner), wo_ss, wo_rs)
    wout_gather.start()
    for load in loads:
        load.wait()
    tok_gather.finish()

    lane = lax.broadcasted_iota(jnp.int32, (LANES, LANES), 1)
    low = lane < HEAD

    qgain = qgain_ref[0:1, :]
    kgain = kgain_ref[0:1, :]

    def head_norm(raw_part, gain):
        square = raw_part * raw_part
        lo = jnp.sum(jnp.where(low, square, 0.0), axis=1, keepdims=True) * (1.0 / HEAD)
        hi = jnp.sum(jnp.where(low, 0.0, square), axis=1, keepdims=True) * (1.0 / HEAD)
        inverse = jnp.where(low, lax.rsqrt(lo + NORM_EPS), lax.rsqrt(hi + NORM_EPS))
        return raw_part * inverse * gain

    @pl.loop(0, blk // LANES)
    def _(t):
        rows = pl.ds(pl.multiple_of(t * LANES, LANES), LANES)
        raw[...] = jnp.dot(tok[rows, :], wqkv[...], preferred_element_type=F32)
        q_part = head_norm(raw[:, 0:width], qgain) * (HEAD**-0.5)
        k_part = head_norm(raw[:, width : 2 * width], kgain)
        v_part = raw[:, 2 * width : 3 * width]
        k_roll = pltpu.roll(k_part, HEAD, 1)
        v_roll = pltpu.roll(v_part, HEAD, 1)
        q_send[0, rows, :] = jnp.where(low, q_part, 0.0).astype(BF16)
        q_send[1, rows, :] = jnp.where(low, pltpu.roll(q_part, HEAD, 1), 0.0).astype(BF16)
        kv_send[0, rows, :] = jnp.where(low, k_part, v_roll).astype(BF16)
        kv_send[1, rows, :] = jnp.where(low, k_roll, v_part).astype(BF16)

    par = lax.rem(y, 2)
    a2a = []
    for i in range(2):
        j = 2 * c + i
        target = device(z, j, x, owner_core)
        own_block = kv_all.at[z, pl.ds(pl.multiple_of(y * blk, blk), blk)]
        parts = (
            (kv_send.at[i], own_block),
            (q_send.at[i], q_recv.at[par]),
            (gates_ref.at[i], gate_recv.at[par]),
        )
        for n, (src, dst) in enumerate(parts):
            send_sem, recv_sem = a2a_ss.at[n, i], a2a_rs.at[n, par]
            remote = pltpu.make_async_remote_copy(
                src_ref=src,
                dst_ref=dst,
                send_sem=send_sem,
                recv_sem=recv_sem,
                device_id=target,
                device_id_type=MESH,
            )
            local = pltpu.make_async_copy(src, dst, recv_sem)

            @pl.when(j != y)
            def _():
                remote.start()

            @pl.when(j == y)
            def _():
                local.start()

            a2a.append((j, remote))

    base = c * half
    for s in range(2):
        src_rows = pl.ds(pl.multiple_of(base + s * blk, blk), blk)
        for n, dst in enumerate((kv_all.at[z, src_rows], q_recv.at[s], gate_recv.at[s])):
            pltpu.make_async_copy(dst, dst, a2a_rs.at[n, s]).wait()

    gate_all[z, c] = gate_recv[0] + gate_recv[1]
    subs = half // SUB

    def kv_piece(b, core, s):
        return kv_all.at[b, pl.ds(pl.multiple_of(core * half + s * SUB, SUB), SUB)]

    def ring_copy(d, b, s, k, target):
        piece = kv_piece(b, c, s)
        return pltpu.make_async_remote_copy(
            src_ref=piece,
            dst_ref=piece,
            send_sem=ring_ss.at[d, k - 1, s],
            recv_sem=ring_rs.at[d, k - 1, s],
            device_id=target,
            device_id_type=MESH,
        )

    def ring_gate(d, b, k, target):
        piece = gate_all.at[b, c]
        return pltpu.make_async_remote_copy(
            src_ref=piece,
            dst_ref=piece,
            send_sem=gring_ss.at[d, k - 1],
            recv_sem=gring_rs.at[d, k - 1],
            device_id=target,
            device_id_type=MESH,
        )

    def d2d_copy(d, b, core, s, k):
        piece = kv_piece(b, core, s)
        return pltpu.make_async_remote_copy(
            src_ref=piece,
            dst_ref=piece,
            send_sem=d2d_ss.at[d, k - 1, s],
            recv_sem=d2d_rs.at[d, k - 1, s],
            device_id=partner,
            device_id_type=MESH,
        )

    def d2d_gate(d, b, core, k):
        piece = gate_all.at[b, core]
        return pltpu.make_async_remote_copy(
            src_ref=piece,
            dst_ref=piece,
            send_sem=gd2d_ss.at[d, k - 1],
            recv_sem=gd2d_rs.at[d, k - 1],
            device_id=partner,
            device_id_type=MESH,
        )

    k_up = nz // 2
    k_down = nz - 1 - k_up
    last_wrapped = k_down - 1
    links = (up, down)

    def block_of(d, k):
        return z - k if d == 0 else lax.rem(z + k, nz)

    def receives(d, k):
        if d == 0:
            return jnp.logical_and(z - k >= 0, k <= k_up)
        return jnp.logical_and(block_of(1, k) <= last_wrapped, k <= k_down)

    def sends(d, k):
        if d == 0:
            return jnp.logical_and(
                jnp.logical_and(z - k + 1 >= 0, z <= nz - 2), k <= k_up
            )
        return jnp.logical_and(block_of(1, k - 1) <= last_wrapped, k <= k_down)

    def needs(d, k):
        if d == 0:
            return receives(0, k)
        return jnp.logical_and(receives(1, k), block_of(1, k) < z)

    def own_copy(core, s):
        piece = kv_piece(z, core, s)
        return pltpu.make_async_remote_copy(
            src_ref=piece,
            dst_ref=piece,
            send_sem=own_ss.at[s],
            recv_sem=own_rs.at[s],
            device_id=partner,
            device_id_type=MESH,
        )

    def own_gate(core):
        piece = gate_all.at[z, core]
        return pltpu.make_async_remote_copy(
            src_ref=piece,
            dst_ref=piece,
            send_sem=own_ss.at[subs],
            recv_sem=own_rs.at[subs],
            device_id=partner,
            device_id_type=MESH,
        )

    for s in range(subs):
        for d in range(2):

            @pl.when(sends(d, 1))
            def _():
                if s == 0:
                    ring_gate(d, z, 1, links[d]).start()
                ring_copy(d, z, s, 1, links[d]).start()

        own_copy(c, s).start()
    own_gate(c).start()

    gate_t = jnp.transpose(gate_all[z, c])
    tiles_blk = blk // LANES
    for s in range(2):
        q_s[pl.ds(s * blk, blk), :] = q_recv[s]
    for t in range(2 * tiles_blk):
        column = gate_t[:, t : t + 1]
        gt_s[pl.ds(t * LANES, LANES), :] = jnp.broadcast_to(column, (LANES, LANES))
    m_s[...] = jnp.full(m_s.shape, -1e30, F32)
    o_s[...] = jnp.zeros(o_s.shape, F32)

    lane_row = lax.broadcasted_iota(jnp.int32, (1, LANES), 1)
    ones_low = jnp.where(lane_row < HEAD, 1.0, 0.0).astype(BF16)
    keep_high = jnp.where(lane_row < HEAD, 0.0, 1.0).astype(BF16)
    lane_tiles = SUB // LANES

    def update(q_tile, pieces, masked_at=None):
        rows = pl.ds(pl.multiple_of(q_tile * QT, QT), QT)
        query = q_s[rows, :]
        gt = gt_s[rows, :]
        m_old = m_s[rows, :]
        scores = []
        peak = None
        for key, gate_row, value in pieces:
            score = lax.dot_general(
                query, key, (((1,), (1,)), ((), ())), preferred_element_type=F32
            )
            score = score - gate_row
            if masked_at is not None:
                row_id, col_id = masked_at
                score = jnp.where(
                    lax.broadcasted_iota(jnp.int32, score.shape, 1) + col_id
                    <= lax.broadcasted_iota(jnp.int32, score.shape, 0) + row_id,
                    score,
                    -jnp.inf,
                )
            scores.append(score)
            top = jnp.max(score, axis=1, keepdims=True)
            peak = top if peak is None else jnp.maximum(peak, top)
        m_new = jnp.maximum(m_old, peak + gt)
        offset = m_new - gt
        wide = jnp.concatenate([offset] * lane_tiles, axis=1)
        total = o_s[rows, :] * jnp.exp(m_old - m_new)
        for (key, gate_row, value), score in zip(pieces, scores):
            probs = jnp.exp(score - wide).astype(BF16)
            total = total + jnp.dot(probs, value, preferred_element_type=F32)
        o_s[rows, :] = total
        m_s[rows, :] = m_new

    def gate_row_of(b, core, s):
        return jnp.concatenate(
            [gate_all[b, core, pl.ds(s * lane_tiles + i, 1), :] for i in range(lane_tiles)],
            axis=1,
        )

    for s in range(subs):
        own_copy(1 - c, s).wait_recv()
    own_gate(1 - c).wait_recv()
    for core in range(2):
        for s in range(subs):

            @pl.when(core <= c)
            def _():
                key = kv_all[z, pl.ds(core * half + s * SUB, SUB), :]
                value = key * keep_high + ones_low
                gate_row = gate_row_of(z, core, s)
                col_id = core * half + s * SUB

                @pl.loop(0, half // QT)
                def _(t):
                    row_id = c * half + t * QT

                    @pl.when(row_id + QT > col_id)
                    def _():
                        update(t, [(key, gate_row, value)], (row_id, col_id))

    def one_chunk(d, k, s):
        @pl.when(needs(d, k))
        def _():
            b = block_of(d, k)
            if s == 0:
                d2d_gate(d, b, 1 - c, k).wait_recv()
            d2d_copy(d, b, 1 - c, s, k).wait_recv()
            for core in range(2):
                key = kv_all[b, pl.ds(core * half + s * SUB, SUB), :]
                v_s[pl.ds(core * SUB, SUB), :] = key * keep_high + ones_low

            @pl.loop(0, half // QT)
            def _(t):
                update(
                    t,
                    [
                        (
                            kv_all[b, pl.ds(core * half + s * SUB, SUB), :],
                            gate_row_of(b, core, s),
                            v_s[pl.ds(core * SUB, SUB), :],
                        )
                        for core in range(2)
                    ],
                )

    def pass_on(d, k, s):
        @pl.when(receives(d, k))
        def _():
            b = block_of(d, k)
            if s == 0:
                ring_gate(d, b, k, links[d]).wait_recv()
            ring_copy(d, b, s, k, links[d]).wait_recv()

            @pl.when(sends(d, k + 1))
            def _():
                if s == 0:
                    ring_gate(d, b, k + 1, links[d]).start()
                ring_copy(d, b, s, k + 1, links[d]).start()

            @pl.when(needs(d, k))
            def _():
                if s == 0:
                    d2d_gate(d, b, c, k).start()
                d2d_copy(d, b, c, s, k).start()

    @pl.loop(1, k_up + 1)
    def _(k):
        for s in range(subs):
            pass_on(0, k, s)
            pass_on(1, k, s)
            if s == 0:

                @pl.when(k > 1)
                def _():
                    one_chunk(0, k - 1, subs - 1)
                    one_chunk(1, k - 1, subs - 1)

            else:
                one_chunk(0, k, s - 1)
                one_chunk(1, k, s - 1)

        @pl.when(k == k_up // 2)
        def _():
            wout_gather.relay()

        @pl.when(k == k_up - 1)
        def _():
            wout_gather.finish_links()

    one_chunk(0, k_up, subs - 1)
    one_chunk(1, k_up, subs - 1)

    odd = lax.rem(y, 2) == 1

    @pl.loop(0, half // LANES)
    def _(t):
        rows = pl.ds(pl.multiple_of(t * LANES, LANES), LANES)
        both = o_s[rows, :]
        swapped = pltpu.roll(both, HEAD, 1)

        @pl.when(odd)
        def _():
            att_send[rows, :] = jnp.where(low, 0.0, both / swapped).astype(BF16)

        @pl.when(jnp.logical_not(odd))
        def _():
            att_send[rows, :] = jnp.where(low, swapped / both, 0.0).astype(BF16)

    head = NY * x + y
    att = []
    for s in range(2):
        for t in range(NX * NC):
            ty = 2 * c + s
            src = att_send.at[pl.ds(s * blk + t * rows_tp, rows_tp)]
            remote = pltpu.make_async_remote_copy(
                src_ref=src,
                dst_ref=att_recv.at[head],
                send_sem=att_ss.at[s * NX * NC + t],
                recv_sem=att_rs.at[head],
                device_id=(z * NY + ty, t),
                device_id_type=MESH,
            )
            local = pltpu.make_async_copy(src, att_recv.at[head], att_rs.at[head])
            is_self = jnp.logical_and(ty == y, tp == t)

            @pl.when(jnp.logical_not(is_self))
            def _():
                remote.start()

            @pl.when(is_self)
            def _():
                local.start()

            att.append((is_self, remote))

    wout_gather.finish()
    for h in range(NX * NY):
        pltpu.make_async_copy(att_recv.at[h], att_recv.at[h], att_rs.at[h]).wait()

    groups = NX * NC
    pairs = [att_recv[2 * g] + att_recv[2 * g + 1] for g in range(groups)]
    cols = 256

    @pl.loop(0, out_ref.shape[1] // cols)
    def _(t):
        span = pl.ds(pl.multiple_of(t * cols, cols), cols)
        acc = jnp.zeros((rows_tp, cols), F32)
        for g in range(groups):
            part = jnp.dot(
                pairs[g],
                wout[pl.ds(g * wout_rows, wout_rows), span],
                preferred_element_type=F32,
            )
            acc = acc + part.astype(BF16).astype(F32)
        out_ref[:, span] = acc.astype(BF16)

    tok_gather.drain()
    wout_gather.drain()
    for j, remote in a2a:

        @pl.when(j != y)
        def _():
            remote.wait_send()

    for s in range(subs):
        own_copy(c, s).wait_send()
    own_gate(c).wait_send()

    @pl.loop(1, k_up + 1)
    def _(k):
        for d in range(2):

            @pl.when(sends(d, k))
            def _():
                b = block_of(d, k - 1)
                ring_gate(d, b, k, links[d]).wait_send()
                for s in range(subs):
                    ring_copy(d, b, s, k, links[d]).wait_send()

            @pl.when(needs(d, k))
            def _():
                b = block_of(d, k)
                d2d_gate(d, b, c, k).wait_send()
                for s in range(subs):
                    d2d_copy(d, b, c, s, k).wait_send()

    for is_self, remote in att:

        @pl.when(jnp.logical_not(is_self))
        def _():
            remote.wait_send()


def on_device(
    nz,
    tokens,
    query_weight,
    key_weight,
    value_weight,
    query_gain,
    key_gain,
    log_gate_total,
    output_weight,
):
    rows_tp, depth = tokens.shape
    width = query_weight.shape[1]
    blk, heads = log_gate_total.shape
    half = 2 * blk
    tiles = blk // LANES
    y = lax.rem(lax.axis_index("sp"), NY)
    rows = log_gate_total.T.reshape(heads, tiles, LANES)
    empty = jnp.zeros_like(rows)
    rest = jnp.zeros((heads, 8 - 2 * tiles, LANES), F32)
    odd = (y % 2) == 1
    gates = jnp.concatenate(
        [jnp.where(odd, empty, rows), jnp.where(odd, rows, empty), rest], axis=1
    )
    gain_rows = lambda gain: jnp.broadcast_to(jnp.concatenate([gain, gain])[None, :], (8, LANES))
    k_up = nz // 2
    subs = half // SUB
    dma = pltpu.SemaphoreType.DMA
    any_spec = pl.BlockSpec(memory_space=pl.ANY)
    vmem_spec = pl.BlockSpec(memory_space=pltpu.VMEM)
    return pl.pallas_call(
        functools.partial(kernel, nz),
        out_shape=jax.ShapeDtypeStruct((rows_tp, output_weight.shape[1]), BF16),
        in_specs=[any_spec] * 4 + [vmem_spec] * 3 + [any_spec],
        out_specs=vmem_spec,
        scratch_shapes=[
            pltpu.VMEM((blk, depth), BF16),
            pltpu.VMEM((depth, 3 * width), BF16),
            pltpu.VMEM((NX * NC * output_weight.shape[0], output_weight.shape[1]), BF16),
            pltpu.VMEM((LANES, 3 * width), F32),
            pltpu.VMEM((2, blk, LANES), BF16),
            pltpu.VMEM((2, blk, LANES), BF16),
            pltpu.VMEM((2, blk, LANES), BF16),
            pltpu.VMEM((2, 8, LANES), F32),
            pltpu.VMEM((nz, 2 * half, LANES), BF16),
            pltpu.VMEM((nz, 2, 8, LANES), F32),
            pltpu.VMEM((half, LANES), BF16),
            pltpu.VMEM((half, LANES), F32),
            pltpu.VMEM((half, LANES), F32),
            pltpu.VMEM((half, LANES), F32),
            pltpu.VMEM((2 * SUB, LANES), BF16),
            pltpu.VMEM((half, LANES), BF16),
            pltpu.VMEM((NX * NY, rows_tp, LANES), BF16),
            dma((5,)),
            dma((13,)),
            dma((13,)),
            dma((13,)),
            dma((13,)),
            dma((3, 2)),
            dma((3, 2)),
            dma((2, k_up, subs)),
            dma((2, k_up, subs)),
            dma((2, k_up, subs)),
            dma((2, k_up, subs)),
            dma((2, k_up)),
            dma((2, k_up)),
            dma((2, k_up)),
            dma((2, k_up)),
            dma((subs + 1,)),
            dma((subs + 1,)),
            dma((NX * NY,)),
            dma((NX * NY,)),
        ],
        compiler_params=pltpu.CompilerParams(
            collective_id=0, has_side_effects=True, vmem_limit_bytes=60 * 1024 * 1024
        ),
    )(
        tokens,
        query_weight,
        key_weight,
        value_weight,
        gain_rows(query_gain),
        gain_rows(key_gain),
        gates,
        output_weight,
    )


def solution(mesh):
    placed = (
        P(("sp", "tp"), None),
        P(None, "tp"),
        P(None, "tp"),
        P(None, "tp"),
        P(),
        P(),
        P("sp", "tp"),
        P("tp", None),
    )
    nz = mesh.shape["sp"] // NY
    return jax.shard_map(
        functools.partial(on_device, nz),
        mesh=mesh,
        in_specs=placed,
        out_specs=P(("sp", "tp"), None),
        check_vma=False,
    )
```

```python
import functools

import jax
import jax.numpy as jnp
from jax import lax
from jax.experimental import pallas as pl
from jax.experimental.pallas import tpu as pltpu
from jax.sharding import PartitionSpec as P

NORM_EPS = 1e-06
MESH = pl.DeviceIdType.MESH
F32 = jnp.float32
BF16 = jnp.bfloat16
LANES = 128
HEAD = 64
NX = 4
NY = 4
NC = 2
SUB = 384
QT = 384


class RowGather:
    def __init__(self, buf, rows, x, c, ids, ssem, rsem):
        self.buf, self.rows, self.x, self.c = buf, rows, x, c
        self.right, self.left, self.partner = ids
        self.ssem, self.rsem = ssem, rsem
        self.half = buf.shape[1] // 2

    def piece(self, dx, core, part):
        slot = lax.rem(self.x + dx + NX, NX) * NC + core
        rows = pl.ds(pl.multiple_of(slot * self.rows, self.rows), self.rows)
        if part is None:
            return self.buf.at[rows]
        return self.buf.at[rows, pl.ds(part * self.half, self.half)]

    def copy(self, dx, core, part, index):
        device = self.right if index < 3 else self.left if index < 6 else self.partner
        piece = self.piece(dx, core, part)
        return pltpu.make_async_remote_copy(
            src_ref=piece,
            dst_ref=piece,
            send_sem=self.ssem.at[index],
            recv_sem=self.rsem.at[index],
            device_id=device,
            device_id_type=MESH,
        )

    def send(self, dx, part, index):
        self.copy(dx, self.c, part, index).start()

    def arrive(self, dx, core, part, index):
        self.copy(dx, core, part, index).wait_recv()

    def start(self):
        self.send(0, 0, 0)
        self.send(0, 1, 3)
        self.send(0, 1, 1)
        self.send(0, 0, 4)
        self.send(0, None, 6)

    def relay(self):
        self.arrive(-1, self.c, 0, 0)
        self.send(-1, 0, 2)
        self.arrive(1, self.c, 1, 3)
        self.send(1, 1, 5)
        self.send(-1, 0, 7)
        self.send(1, 1, 8)

    def finish_links(self):
        self.arrive(-1, self.c, 1, 1)
        self.send(-1, 1, 9)
        self.arrive(1, self.c, 0, 4)
        self.send(1, 0, 10)
        self.arrive(-2, self.c, 0, 2)
        self.send(-2, 0, 11)
        self.arrive(2, self.c, 1, 5)
        self.send(2, 1, 12)

    def finish(self):
        other = 1 - self.c
        self.arrive(0, other, None, 6)
        self.arrive(-1, other, 0, 7)
        self.arrive(1, other, 1, 8)
        self.arrive(-1, other, 1, 9)
        self.arrive(1, other, 0, 10)
        self.arrive(-2, other, 0, 11)
        self.arrive(2, other, 1, 12)

    def drain(self):
        sent = [(0, 0, 0), (0, 1, 3), (0, 1, 1), (0, 0, 4), (0, None, 6), (-1, 0, 2), (1, 1, 5)]
        sent += [(-1, 0, 7), (1, 1, 8), (-1, 1, 9), (1, 0, 10), (-2, 0, 11), (2, 1, 12)]
        for dx, part, index in sent:
            self.copy(dx, self.c, part, index).wait_send()


def kernel(
    nz,
    tokens_ref,
    wq_ref,
    wk_ref,
    wv_ref,
    qgain_ref,
    kgain_ref,
    gates_ref,
    wout_ref,
    out_ref,
    tok,
    wqkv,
    wout,
    raw,
    kv_send,
    q_send,
    gain_v,
    gate_v,
    gate_send,
    q_recv,
    gate_recv,
    kv_all,
    gate_all,
    q_s,
    gt_s,
    m_s,
    o_s,
    v_s,
    att_send,
    att_recv,
    lsem,
    tok_ss,
    tok_rs,
    wo_ss,
    wo_rs,
    a2a_ss,
    a2a_rs,
    ring_ss,
    ring_rs,
    d2d_ss,
    d2d_rs,
    gring_ss,
    gring_rs,
    gd2d_ss,
    gd2d_rs,
    own_ss,
    own_rs,
    att_ss,
    att_rs,
):
    sp = lax.axis_index("sp")
    tp = lax.axis_index("tp")
    z, y = lax.div(sp, NY), lax.rem(sp, NY)
    x, c = lax.div(tp, NC), lax.rem(tp, NC)

    def device(dz, dy, dx, dc):
        return (dz * NY + dy, dx * NC + dc)

    right = device(z, y, lax.rem(x + 1, NX), c)
    left = device(z, y, lax.rem(x + NX - 1, NX), c)
    partner = device(z, y, x, 1 - c)
    up = device(lax.rem(z + 1, nz), y, x, c)
    down = device(lax.rem(z + nz - 1, nz), y, x, c)
    owner_core = lax.div(y, 2)

    rows_tp = tokens_ref.shape[0]
    blk = rows_tp * NX * NC
    half = 2 * blk
    width = wq_ref.shape[1]

    own_rows = pl.ds(pl.multiple_of(tp * rows_tp, rows_tp), rows_tp)
    wout_rows = wout_ref.shape[0]
    load_tok = pltpu.make_async_copy(tokens_ref, tok.at[own_rows], lsem.at[0])
    load_tok.start()
    loads = []
    for i, w_ref in enumerate((wq_ref, wk_ref, wv_ref)):
        loads.append(
            pltpu.make_async_copy(w_ref, wqkv.at[:, pl.ds(i * width, width)], lsem.at[1 + i])
        )
    load_wout = pltpu.make_async_copy(
        wout_ref,
        wout.at[pl.ds(pl.multiple_of(tp * wout_rows, wout_rows), wout_rows)],
        lsem.at[4],
    )
    for load in loads:
        load.start()
    load_wout.start()
    smalls = []
    for i, (src, dst) in enumerate(
        ((qgain_ref, gain_v.at[0]), (kgain_ref, gain_v.at[1]), (gates_ref, gate_v))
    ):
        smalls.append(pltpu.make_async_copy(src, dst, lsem.at[5 + i]))
        smalls[-1].start()

    barrier = pltpu.get_barrier_semaphore()
    for neighbour in (right, left, partner, up, down):
        pl.semaphore_signal(barrier, inc=1, device_id=neighbour, device_id_type=MESH)
    for i in range(2):
        j = 2 * c + i

        @pl.when(j != y)
        def _():
            pl.semaphore_signal(
                barrier, inc=1, device_id=device(z, j, x, owner_core), device_id_type=MESH
            )

    @pl.when(owner_core == c)
    def _():
        pl.semaphore_wait(barrier, 6)

    @pl.when(owner_core != c)
    def _():
        pl.semaphore_wait(barrier, 7)

    load_tok.wait()
    tok_gather = RowGather(tok, rows_tp, x, c, (right, left, partner), tok_ss, tok_rs)
    tok_gather.start()
    tok_gather.relay()
    tok_gather.finish_links()
    load_wout.wait()
    wout_gather = RowGather(wout, wout_rows, x, c, (right, left, partner), wo_ss, wo_rs)
    wout_gather.start()
    for load in loads:
        load.wait()
    tok_gather.finish()

    lane = lax.broadcasted_iota(jnp.int32, (LANES, LANES), 1)
    low = lane < HEAD

    for small in smalls:
        small.wait()
    qgain, kgain = [jnp.concatenate([gain_v[i], gain_v[i]], axis=1) for i in range(2)]
    par = lax.rem(y, 2)
    tiles_blk = blk // LANES
    sublane = lax.broadcasted_iota(jnp.int32, (8, LANES), 0)
    for i in range(2):
        tile = jnp.zeros((8, LANES), F32)
        for t in range(tiles_blk):
            row = jnp.broadcast_to(gate_v[i : i + 1, t * LANES : (t + 1) * LANES], (8, LANES))
            tile = jnp.where(sublane == par * tiles_blk + t, row, tile)
        gate_send[i] = tile

    def head_norm(raw_part, gain):
        square = raw_part * raw_part
        lo = jnp.sum(jnp.where(low, square, 0.0), axis=1, keepdims=True) * (1.0 / HEAD)
        hi = jnp.sum(jnp.where(low, 0.0, square), axis=1, keepdims=True) * (1.0 / HEAD)
        inverse = jnp.where(low, lax.rsqrt(lo + NORM_EPS), lax.rsqrt(hi + NORM_EPS))
        return raw_part * inverse * gain

    @pl.loop(0, blk // LANES)
    def _(t):
        rows = pl.ds(pl.multiple_of(t * LANES, LANES), LANES)
        raw[...] = jnp.dot(tok[rows, :], wqkv[...], preferred_element_type=F32)
        q_part = head_norm(raw[:, 0:width], qgain) * (HEAD**-0.5)
        k_part = head_norm(raw[:, width : 2 * width], kgain)
        v_part = raw[:, 2 * width : 3 * width]
        k_roll = pltpu.roll(k_part, HEAD, 1)
        v_roll = pltpu.roll(v_part, HEAD, 1)
        q_send[0, rows, :] = jnp.where(low, q_part, 0.0).astype(BF16)
        q_send[1, rows, :] = jnp.where(low, pltpu.roll(q_part, HEAD, 1), 0.0).astype(BF16)
        kv_send[0, rows, :] = jnp.where(low, k_part, v_roll).astype(BF16)
        kv_send[1, rows, :] = jnp.where(low, k_roll, v_part).astype(BF16)

    a2a = []
    for i in range(2):
        j = 2 * c + i
        target = device(z, j, x, owner_core)
        own_block = kv_all.at[z, pl.ds(pl.multiple_of(y * blk, blk), blk)]
        parts = (
            (kv_send.at[i], own_block),
            (q_send.at[i], q_recv.at[par]),
            (gate_send.at[i], gate_recv.at[par]),
        )
        for n, (src, dst) in enumerate(parts):
            send_sem, recv_sem = a2a_ss.at[n, i], a2a_rs.at[n, par]
            remote = pltpu.make_async_remote_copy(
                src_ref=src,
                dst_ref=dst,
                send_sem=send_sem,
                recv_sem=recv_sem,
                device_id=target,
                device_id_type=MESH,
            )
            local = pltpu.make_async_copy(src, dst, recv_sem)

            @pl.when(j != y)
            def _():
                remote.start()

            @pl.when(j == y)
            def _():
                local.start()

            a2a.append((j, remote))

    base = c * half
    for s in range(2):
        src_rows = pl.ds(pl.multiple_of(base + s * blk, blk), blk)
        for n, dst in enumerate((kv_all.at[z, src_rows], q_recv.at[s], gate_recv.at[s])):
            pltpu.make_async_copy(dst, dst, a2a_rs.at[n, s]).wait()

    gate_all[z, c] = gate_recv[0] + gate_recv[1]
    subs = half // SUB

    def kv_piece(b, core, s):
        return kv_all.at[b, pl.ds(pl.multiple_of(core * half + s * SUB, SUB), SUB)]

    def ring_copy(d, b, s, k, target):
        piece = kv_piece(b, c, s)
        return pltpu.make_async_remote_copy(
            src_ref=piece,
            dst_ref=piece,
            send_sem=ring_ss.at[d, k - 1, s],
            recv_sem=ring_rs.at[d, k - 1, s],
            device_id=target,
            device_id_type=MESH,
        )

    def ring_gate(d, b, k, target):
        piece = gate_all.at[b, c]
        return pltpu.make_async_remote_copy(
            src_ref=piece,
            dst_ref=piece,
            send_sem=gring_ss.at[d, k - 1],
            recv_sem=gring_rs.at[d, k - 1],
            device_id=target,
            device_id_type=MESH,
        )

    def d2d_copy(d, b, core, s, k):
        piece = kv_piece(b, core, s)
        return pltpu.make_async_remote_copy(
            src_ref=piece,
            dst_ref=piece,
            send_sem=d2d_ss.at[d, k - 1, s],
            recv_sem=d2d_rs.at[d, k - 1, s],
            device_id=partner,
            device_id_type=MESH,
        )

    def d2d_gate(d, b, core, k):
        piece = gate_all.at[b, core]
        return pltpu.make_async_remote_copy(
            src_ref=piece,
            dst_ref=piece,
            send_sem=gd2d_ss.at[d, k - 1],
            recv_sem=gd2d_rs.at[d, k - 1],
            device_id=partner,
            device_id_type=MESH,
        )

    k_up = nz // 2
    k_down = nz - 1 - k_up
    last_wrapped = k_down - 1
    links = (up, down)

    def block_of(d, k):
        return z - k if d == 0 else lax.rem(z + k, nz)

    def receives(d, k):
        if d == 0:
            return jnp.logical_and(z - k >= 0, k <= k_up)
        return jnp.logical_and(block_of(1, k) <= last_wrapped, k <= k_down)

    def sends(d, k):
        if d == 0:
            return jnp.logical_and(
                jnp.logical_and(z - k + 1 >= 0, z <= nz - 2), k <= k_up
            )
        return jnp.logical_and(block_of(1, k - 1) <= last_wrapped, k <= k_down)

    def needs(d, k):
        if d == 0:
            return receives(0, k)
        return jnp.logical_and(receives(1, k), block_of(1, k) < z)

    def own_copy(core, s):
        piece = kv_piece(z, core, s)
        return pltpu.make_async_remote_copy(
            src_ref=piece,
            dst_ref=piece,
            send_sem=own_ss.at[s],
            recv_sem=own_rs.at[s],
            device_id=partner,
            device_id_type=MESH,
        )

    def own_gate(core):
        piece = gate_all.at[z, core]
        return pltpu.make_async_remote_copy(
            src_ref=piece,
            dst_ref=piece,
            send_sem=own_ss.at[subs],
            recv_sem=own_rs.at[subs],
            device_id=partner,
            device_id_type=MESH,
        )

    for s in range(subs):
        for d in range(2):

            @pl.when(sends(d, 1))
            def _():
                if s == 0:
                    ring_gate(d, z, 1, links[d]).start()
                ring_copy(d, z, s, 1, links[d]).start()

    @pl.when(c == 0)
    def _():
        for s in range(subs):
            own_copy(c, s).start()
        own_gate(c).start()


    gate_t = jnp.transpose(gate_all[z, c])
    for s in range(2):
        q_s[pl.ds(s * blk, blk), :] = q_recv[s]
    for t in range(2 * tiles_blk):
        column = gate_t[:, t : t + 1]
        gt_s[pl.ds(t * LANES, LANES), :] = jnp.broadcast_to(column, (LANES, LANES))
    m_s[...] = jnp.full(m_s.shape, -1e30, F32)
    o_s[...] = jnp.zeros(o_s.shape, F32)

    lane_row = lax.broadcasted_iota(jnp.int32, (1, LANES), 1)
    ones_low = jnp.where(lane_row < HEAD, 1.0, 0.0).astype(BF16)
    keep_high = jnp.where(lane_row < HEAD, 0.0, 1.0).astype(BF16)
    tiles = half // QT

    def update(b, cores, masked=False):
        count = len(cores) * half
        if count == 2 * half:
            keys = lambda: kv_all[b]
        else:
            first = pl.multiple_of(cores[0] * half, half)
            keys = lambda: kv_all[b, pl.ds(first, half), :]
        v_s[pl.ds(0, count), :] = keys() * keep_high + ones_low
        gate_row = jnp.concatenate(
            [gate_all[b, core, pl.ds(i, 1), :] for core in cores for i in range(half // LANES)],
            axis=1,
        )

        def score_of(t):
            score = lax.dot_general(
                q_s[pl.ds(t * QT, QT), :],
                keys(),
                (((1,), (1,)), ((), ())),
                preferred_element_type=F32,
            )
            score = score - gate_row
            if masked:
                shape = score.shape
                row_id = lax.broadcasted_iota(jnp.int32, shape, 0) + t * QT
                score = jnp.where(
                    lax.broadcasted_iota(jnp.int32, shape, 1) <= row_id, score, -jnp.inf
                )
            return score

        def add(t, score):
            rows = pl.ds(t * QT, QT)
            gt = gt_s[rows, :]
            m_old = m_s[rows, :]
            m_new = jnp.maximum(m_old, jnp.max(score, axis=1, keepdims=True) + gt)
            wide = jnp.concatenate([m_new - gt] * (count // LANES), axis=1)
            probs = jnp.exp(score - wide).astype(BF16)
            o_s[rows, :] = o_s[rows, :] * jnp.exp(m_old - m_new) + jnp.dot(
                probs, v_s[pl.ds(0, count), :], preferred_element_type=F32
            )
            m_s[rows, :] = m_new

        score = score_of(0)
        for t in range(tiles):
            following = score_of(t + 1) if t + 1 < tiles else None
            add(t, score)
            score = following

    update(z, (c,), masked=True)

    @pl.when(c == 1)
    def _():
        for s in range(subs):
            own_copy(0, s).wait_recv()
        own_gate(0).wait_recv()
        update(z, (1 - c,))

    def one_block(d, k):
        @pl.when(needs(d, k))
        def _():
            b = block_of(d, k)
            d2d_gate(d, b, 1 - c, k).wait_recv()
            for s in range(subs):
                d2d_copy(d, b, 1 - c, s, k).wait_recv()
            update(b, (0, 1))

    def pass_on(d, k, s):
        @pl.when(receives(d, k))
        def _():
            b = block_of(d, k)
            if s == 0:
                ring_gate(d, b, k, links[d]).wait_recv()
            ring_copy(d, b, s, k, links[d]).wait_recv()

            @pl.when(sends(d, k + 1))
            def _():
                if s == 0:
                    ring_gate(d, b, k + 1, links[d]).start()
                ring_copy(d, b, s, k + 1, links[d]).start()

            @pl.when(needs(d, k))
            def _():
                if s == 0:
                    d2d_gate(d, b, c, k).start()
                d2d_copy(d, b, c, s, k).start()

    @pl.loop(1, k_up + 1)
    def _(k):
        for s in range(subs):
            pass_on(0, k, s)
            pass_on(1, k, s)

            @pl.when(k > 1)
            def _():
                one_block(s, k - 1)

        @pl.when(k == k_up // 2)
        def _():
            wout_gather.relay()

        @pl.when(k == k_up - 1)
        def _():
            wout_gather.finish_links()

    one_block(0, k_up)

    odd = lax.rem(y, 2) == 1

    @pl.loop(0, half // LANES)
    def _(t):
        rows = pl.ds(pl.multiple_of(t * LANES, LANES), LANES)
        both = o_s[rows, :]
        swapped = pltpu.roll(both, HEAD, 1)

        @pl.when(odd)
        def _():
            att_send[rows, :] = jnp.where(low, 0.0, both / swapped).astype(BF16)

        @pl.when(jnp.logical_not(odd))
        def _():
            att_send[rows, :] = jnp.where(low, swapped / both, 0.0).astype(BF16)

    head = NY * x + y
    att = []
    for s in range(2):
        for t in range(NX * NC):
            ty = 2 * c + s
            src = att_send.at[pl.ds(s * blk + t * rows_tp, rows_tp)]
            remote = pltpu.make_async_remote_copy(
                src_ref=src,
                dst_ref=att_recv.at[head],
                send_sem=att_ss.at[s * NX * NC + t],
                recv_sem=att_rs.at[head],
                device_id=(z * NY + ty, t),
                device_id_type=MESH,
            )
            local = pltpu.make_async_copy(src, att_recv.at[head], att_rs.at[head])
            is_self = jnp.logical_and(ty == y, tp == t)

            @pl.when(jnp.logical_not(is_self))
            def _():
                remote.start()

            @pl.when(is_self)
            def _():
                local.start()

            att.append((is_self, remote))

    wout_gather.finish()
    for h in range(NX * NY):
        pltpu.make_async_copy(att_recv.at[h], att_recv.at[h], att_rs.at[h]).wait()

    groups = NX * NC
    pairs = [att_recv[2 * g] + att_recv[2 * g + 1] for g in range(groups)]
    cols = 256

    @pl.loop(0, out_ref.shape[1] // cols)
    def _(t):
        span = pl.ds(pl.multiple_of(t * cols, cols), cols)
        acc = jnp.zeros((rows_tp, cols), F32)
        for g in range(groups):
            part = jnp.dot(
                pairs[g],
                wout[pl.ds(g * wout_rows, wout_rows), span],
                preferred_element_type=F32,
            )
            acc = acc + part.astype(BF16).astype(F32)
        out_ref[:, span] = acc.astype(BF16)

    tok_gather.drain()
    wout_gather.drain()
    for j, remote in a2a:

        @pl.when(j != y)
        def _():
            remote.wait_send()

    @pl.when(c == 0)
    def _():
        for s in range(subs):
            own_copy(c, s).wait_send()
        own_gate(c).wait_send()

    @pl.loop(1, k_up + 1)
    def _(k):
        for d in range(2):

            @pl.when(sends(d, k))
            def _():
                b = block_of(d, k - 1)
                ring_gate(d, b, k, links[d]).wait_send()
                for s in range(subs):
                    ring_copy(d, b, s, k, links[d]).wait_send()

            @pl.when(needs(d, k))
            def _():
                b = block_of(d, k)
                d2d_gate(d, b, c, k).wait_send()
                for s in range(subs):
                    d2d_copy(d, b, c, s, k).wait_send()

    for is_self, remote in att:

        @pl.when(jnp.logical_not(is_self))
        def _():
            remote.wait_send()


def on_device(
    nz,
    tokens,
    query_weight,
    key_weight,
    value_weight,
    query_gain,
    key_gain,
    log_gate_total,
    output_weight,
):
    rows_tp, depth = tokens.shape
    width = query_weight.shape[1]
    blk, heads = log_gate_total.shape
    half = 2 * blk
    k_up = nz // 2
    subs = half // SUB
    dma = pltpu.SemaphoreType.DMA
    any_spec = pl.BlockSpec(memory_space=pl.ANY)
    vmem_spec = pl.BlockSpec(memory_space=pltpu.VMEM)
    return pl.pallas_call(
        functools.partial(kernel, nz),
        out_shape=jax.ShapeDtypeStruct((rows_tp, output_weight.shape[1]), BF16),
        in_specs=[any_spec] * 8,
        out_specs=vmem_spec,
        scratch_shapes=[
            pltpu.VMEM((blk, depth), BF16),
            pltpu.VMEM((depth, 3 * width), BF16),
            pltpu.VMEM((NX * NC * output_weight.shape[0], output_weight.shape[1]), BF16),
            pltpu.VMEM((LANES, 3 * width), F32),
            pltpu.VMEM((2, blk, LANES), BF16),
            pltpu.VMEM((2, blk, LANES), BF16),
            pltpu.VMEM((2, 1, HEAD), F32),
            pltpu.VMEM((heads, blk), F32),
            pltpu.VMEM((2, 8, LANES), F32),
            pltpu.VMEM((2, blk, LANES), BF16),
            pltpu.VMEM((2, 8, LANES), F32),
            pltpu.VMEM((nz, 2 * half, LANES), BF16),
            pltpu.VMEM((nz, 2, 8, LANES), F32),
            pltpu.VMEM((half, LANES), BF16),
            pltpu.VMEM((half, LANES), F32),
            pltpu.VMEM((half, LANES), F32),
            pltpu.VMEM((half, LANES), F32),
            pltpu.VMEM((2 * half, LANES), BF16),
            pltpu.VMEM((half, LANES), BF16),
            pltpu.VMEM((NX * NY, rows_tp, LANES), BF16),
            dma((8,)),
            dma((13,)),
            dma((13,)),
            dma((13,)),
            dma((13,)),
            dma((3, 2)),
            dma((3, 2)),
            dma((2, k_up, subs)),
            dma((2, k_up, subs)),
            dma((2, k_up, subs)),
            dma((2, k_up, subs)),
            dma((2, k_up)),
            dma((2, k_up)),
            dma((2, k_up)),
            dma((2, k_up)),
            dma((subs + 1,)),
            dma((subs + 1,)),
            dma((NX * NY,)),
            dma((NX * NY,)),
        ],
        compiler_params=pltpu.CompilerParams(
            collective_id=0, has_side_effects=True, vmem_limit_bytes=60 * 1024 * 1024
        ),
    )(
        tokens,
        query_weight,
        key_weight,
        value_weight,
        query_gain[None, :],
        key_gain[None, :],
        log_gate_total.T,
        output_weight,
    )


def solution(mesh):
    placed = (
        P(("sp", "tp"), None),
        P(None, "tp"),
        P(None, "tp"),
        P(None, "tp"),
        P(),
        P(),
        P("sp", "tp"),
        P("tp", None),
    )
    nz = mesh.shape["sp"] // NY
    return jax.shard_map(
        functools.partial(on_device, nz),
        mesh=mesh,
        in_specs=placed,
        out_specs=P(("sp", "tp"), None),
        check_vma=False,
    )
```

```python
import functools

import jax
import jax.numpy as jnp
from jax import lax
from jax.experimental import pallas as pl
from jax.experimental.pallas import tpu as pltpu
from jax.sharding import PartitionSpec as P

NORM_EPS = 1e-06
MESH = pl.DeviceIdType.MESH
F32 = jnp.float32
BF16 = jnp.bfloat16
LANES = 128
HEAD = 64
NX = 4
NY = 4
NC = 2
QT = 384


class RowGather:
    def __init__(self, buf, rows, x, c, ids, ssem, rsem):
        self.buf, self.rows, self.x, self.c = buf, rows, x, c
        self.right, self.left, self.partner = ids
        self.ssem, self.rsem = ssem, rsem
        self.half = buf.shape[1] // 2

    def piece(self, dx, core, part):
        slot = lax.rem(self.x + dx + NX, NX) * NC + core
        rows = pl.ds(pl.multiple_of(slot * self.rows, self.rows), self.rows)
        if part is None:
            return self.buf.at[rows]
        return self.buf.at[rows, pl.ds(part * self.half, self.half)]

    def copy(self, dx, core, part, index):
        device = self.right if index < 3 else self.left if index < 6 else self.partner
        piece = self.piece(dx, core, part)
        return pltpu.make_async_remote_copy(
            src_ref=piece,
            dst_ref=piece,
            send_sem=self.ssem,
            recv_sem=self.rsem.at[index],
            device_id=device,
            device_id_type=MESH,
        )

    def send(self, dx, part, index):
        self.copy(dx, self.c, part, index).start()

    def arrive(self, dx, core, part, index):
        self.copy(dx, core, part, index).wait_recv()

    def start(self):
        self.send(0, 0, 0)
        self.send(0, 1, 3)
        self.send(0, 1, 1)
        self.send(0, 0, 4)
        self.send(0, None, 6)

    def relay(self):
        self.arrive(-1, self.c, 0, 0)
        self.send(-1, 0, 2)
        self.arrive(1, self.c, 1, 3)
        self.send(1, 1, 5)
        self.send(-1, 0, 7)
        self.send(1, 1, 8)

    def finish_links(self):
        self.arrive(-1, self.c, 1, 1)
        self.send(-1, 1, 9)
        self.arrive(1, self.c, 0, 4)
        self.send(1, 0, 10)
        self.arrive(-2, self.c, 0, 2)
        self.send(-2, 0, 11)
        self.arrive(2, self.c, 1, 5)
        self.send(2, 1, 12)

    def finish(self):
        other = 1 - self.c
        self.arrive(0, other, None, 6)
        self.arrive(-1, other, 0, 7)
        self.arrive(1, other, 1, 8)
        self.arrive(-1, other, 1, 9)
        self.arrive(1, other, 0, 10)
        self.arrive(-2, other, 0, 11)
        self.arrive(2, other, 1, 12)

    def drain(self):
        sent = self.buf.at[pl.ds(0, 7 * self.rows)]
        pltpu.make_async_copy(sent, sent, self.ssem).wait()


def kernel(
    nz,
    tokens_ref,
    wq_ref,
    wk_ref,
    wv_ref,
    qgain_ref,
    kgain_ref,
    gates_ref,
    wout_ref,
    out_ref,
    tok,
    wqkv,
    wout,
    raw,
    kv_send,
    q_send,
    gain_v,
    gate_v,
    gate_send,
    q_recv,
    gate_recv,
    kv_all,
    gate_all,
    q_s,
    gt_s,
    m_s,
    o_s,
    v_s,
    att_send,
    att_recv,
    lsem,
    tok_ss,
    tok_rs,
    wo_ss,
    wo_rs,
    a2a_ss,
    a2a_rs,
    ring_ss,
    ring_rs,
    d2d_ss,
    d2d_rs,
    own_ss,
    own_rs,
    att_ss,
    att_rs,
):
    sp = lax.axis_index("sp")
    tp = lax.axis_index("tp")
    z, y = lax.div(sp, NY), lax.rem(sp, NY)
    x, c = lax.div(tp, NC), lax.rem(tp, NC)

    def device(dz, dy, dx, dc):
        return (dz * NY + dy, dx * NC + dc)

    right = device(z, y, lax.rem(x + 1, NX), c)
    left = device(z, y, lax.rem(x + NX - 1, NX), c)
    partner = device(z, y, x, 1 - c)
    up = device(lax.rem(z + 1, nz), y, x, c)
    down = device(lax.rem(z + nz - 1, nz), y, x, c)
    owner_core = lax.div(y, 2)

    rows_tp = tokens_ref.shape[0]
    blk = rows_tp * NX * NC
    half = 2 * blk
    width = wq_ref.shape[1]

    own_rows = pl.ds(pl.multiple_of(tp * rows_tp, rows_tp), rows_tp)
    wout_rows = wout_ref.shape[0]
    load_tok = pltpu.make_async_copy(tokens_ref, tok.at[own_rows], lsem.at[0])
    load_tok.start()
    loads = []
    for i, w_ref in enumerate((wq_ref, wk_ref, wv_ref)):
        loads.append(
            pltpu.make_async_copy(w_ref, wqkv.at[:, pl.ds(i * width, width)], lsem.at[1 + i])
        )
    load_wout = pltpu.make_async_copy(
        wout_ref,
        wout.at[pl.ds(pl.multiple_of(tp * wout_rows, wout_rows), wout_rows)],
        lsem.at[4],
    )
    for load in loads:
        load.start()
    load_wout.start()
    smalls = []
    for i, (src, dst) in enumerate(
        ((qgain_ref, gain_v.at[0]), (kgain_ref, gain_v.at[1]), (gates_ref, gate_v))
    ):
        smalls.append(pltpu.make_async_copy(src, dst, lsem.at[5 + i]))
        smalls[-1].start()

    barrier = pltpu.get_barrier_semaphore()
    for neighbour in (right, left, partner, up, down):
        pl.semaphore_signal(barrier, inc=1, device_id=neighbour, device_id_type=MESH)
    for i in range(2):
        j = 2 * c + i

        @pl.when(j != y)
        def _():
            pl.semaphore_signal(
                barrier, inc=1, device_id=device(z, j, x, owner_core), device_id_type=MESH
            )

    @pl.when(owner_core == c)
    def _():
        pl.semaphore_wait(barrier, 6)

    @pl.when(owner_core != c)
    def _():
        pl.semaphore_wait(barrier, 7)

    load_tok.wait()
    tok_gather = RowGather(tok, rows_tp, x, c, (right, left, partner), tok_ss, tok_rs)
    tok_gather.start()
    par = lax.rem(y, 2)
    tiles_blk = blk // LANES

    for small in smalls:
        small.wait()
    sublane = lax.broadcasted_iota(jnp.int32, (8, LANES), 0)
    for i in range(2):
        tile = jnp.zeros((8, LANES), F32)
        for t in range(tiles_blk):
            row = jnp.broadcast_to(gate_v[i : i + 1, t * LANES : (t + 1) * LANES], (8, LANES))
            tile = jnp.where(sublane == par * tiles_blk + t, row, tile)
        gate_send[i] = tile

    def exchange(n, i, src, dst):
        j = 2 * c + i
        remote = pltpu.make_async_remote_copy(
            src_ref=src,
            dst_ref=dst,
            send_sem=a2a_ss.at[n, i],
            recv_sem=a2a_rs.at[n, par],
            device_id=device(z, j, x, owner_core),
            device_id_type=MESH,
        )

        @pl.when(j != y)
        def _():
            remote.start()

        @pl.when(j == y)
        def _():
            pltpu.make_async_copy(src, dst, a2a_rs.at[n, par]).start()

        exchanged.append((j, remote))

    def received(n, s, dst):
        pltpu.make_async_copy(dst, dst, a2a_rs.at[n, s]).wait()

    exchanged = []
    for i in range(2):
        exchange(2, i, gate_send.at[i], gate_recv.at[par])

    tok_gather.relay()
    tok_gather.finish_links()
    load_wout.wait()
    wout_gather = RowGather(wout, wout_rows, x, c, (right, left, partner), wo_ss, wo_rs)
    wout_gather.start()
    for load in loads:
        load.wait()
    tok_gather.finish()

    lane = lax.broadcasted_iota(jnp.int32, (LANES, LANES), 1)
    low = lane < HEAD
    qgain, kgain = [jnp.concatenate([gain_v[i], gain_v[i]], axis=1) for i in range(2)]

    def head_norm(raw_part, gain):
        square = raw_part * raw_part
        lo = jnp.sum(jnp.where(low, square, 0.0), axis=1, keepdims=True) * (1.0 / HEAD)
        hi = jnp.sum(jnp.where(low, 0.0, square), axis=1, keepdims=True) * (1.0 / HEAD)
        inverse = jnp.where(low, lax.rsqrt(lo + NORM_EPS), lax.rsqrt(hi + NORM_EPS))
        return raw_part * inverse * gain

    raw[...] = jnp.dot(tok[...], wqkv[:, width : 3 * width], preferred_element_type=F32)
    for t in range(tiles_blk):
        rows = pl.ds(t * LANES, LANES)
        k_part = head_norm(raw[rows, 0:width], kgain)
        v_part = raw[rows, width : 2 * width]
        k_roll = pltpu.roll(k_part, HEAD, 1)
        v_roll = pltpu.roll(v_part, HEAD, 1)
        kv_send[0, rows, :] = jnp.where(low, k_part, v_roll).astype(BF16)
        kv_send[1, rows, :] = jnp.where(low, k_roll, v_part).astype(BF16)
    for i in range(2):
        exchange(0, i, kv_send.at[i], kv_all.at[z, par, owner_core])

    raw[:, 0:width] = jnp.dot(tok[...], wqkv[:, 0:width], preferred_element_type=F32)
    for t in range(tiles_blk):
        rows = pl.ds(t * LANES, LANES)
        raw[rows, width : 2 * width] = head_norm(raw[rows, 0:width], qgain) * (HEAD**-0.5)
    pack = blk // 2
    step = 64
    for t in range(pack // step):
        first = raw[pl.ds(t * step, step), width : 2 * width]
        second = raw[pl.ds(pack + t * step, step), width : 2 * width]
        rows = pl.ds(t * step, step)
        q_send[0, rows, :] = jnp.where(low[:step], first, pltpu.roll(second, HEAD, 1)).astype(BF16)
        q_send[1, rows, :] = jnp.where(low[:step], pltpu.roll(first, HEAD, 1), second).astype(BF16)
    for i in range(2):
        exchange(1, i, q_send.at[i], q_recv.at[par])

    subs = 2

    def chunk_copies(b, s, target, send_sem, recv_sem):
        pieces = (kv_all.at[b, s, c], gate_all.at[b, c])
        return [
            pltpu.make_async_remote_copy(
                src_ref=piece,
                dst_ref=piece,
                send_sem=send_sem,
                recv_sem=recv_sem,
                device_id=target,
                device_id_type=MESH,
            )
            for piece in (pieces if s == 0 else pieces[:1])
        ]

    def chunk_wait(s, sem):
        gate_rows = 8 * LANES * 4 // (LANES * 2)
        sized = v_s.at[pl.ds(0, blk + gate_rows if s == 0 else blk)]
        pltpu.make_async_copy(sized, sized, sem).wait()

    k_up = nz // 2
    links = (up, down)

    def block_of(d, k):
        return z - k if d == 0 else lax.rem(z + k, nz)

    def whole(d, k, s):
        return k <= (k_up if s == d else k_up - 1)

    def highest(s):
        return k_up - 1 if s == 1 else k_up - 2

    def receives(d, k, s):
        block = block_of(d, k)
        return jnp.logical_and(block >= 0 if d == 0 else block <= highest(s), whole(d, k, s))

    def sends(d, k, s):
        if d == 0:
            there = jnp.logical_and(z - k + 1 >= 0, z <= nz - 2)
        else:
            there = lax.rem(z + k - 1, nz) <= highest(s)
        return jnp.logical_and(there, whole(d, k, s))

    def needs(d, k, s):
        if d == 0:
            return receives(0, k, s)
        return jnp.logical_and(receives(1, k, s), block_of(1, k) < z)

    for s in range(subs):
        received(2, s, gate_recv.at[s])
    gate_all[z, c] = gate_recv[0] + gate_recv[1]
    for s in range(subs):
        received(0, s, kv_all.at[z, s, c])
        for d in range(2):

            @pl.when(sends(d, 1, s))
            def _():
                for copy in chunk_copies(z, s, links[d], ring_ss.at[d, s], ring_rs.at[d, 0, s]):
                    copy.start()

    @pl.when(c == 0)
    def _():
        for s in range(subs):
            for copy in chunk_copies(z, s, partner, own_ss.at[s], own_rs.at[s]):
                copy.start()

    gate_t = jnp.transpose(gate_all[z, c])
    for t in range(2 * tiles_blk):
        column = gate_t[:, t : t + 1]
        gt_s[pl.ds(t * LANES, LANES), :] = jnp.broadcast_to(column, (LANES, LANES))
    m_s[...] = jnp.full(m_s.shape, -1e30, F32)
    o_s[...] = jnp.zeros(o_s.shape, F32)
    for s in range(subs):
        received(1, s, q_recv.at[s])
        for t in range(pack // step):
            packed = q_recv[s, pl.ds(t * step, step), :].astype(F32)
            second = pltpu.roll(packed, HEAD, 1)
            for n, rows in enumerate((packed, second)):
                first_row = s * blk + n * pack + t * step
                q_s[pl.ds(first_row, step), :] = jnp.where(low[:step], rows, 0.0).astype(BF16)

    lane_row = lax.broadcasted_iota(jnp.int32, (1, LANES), 1)
    ones_low = jnp.where(lane_row < HEAD, 1.0, 0.0).astype(BF16)
    keep_high = jnp.where(lane_row < HEAD, 0.0, 1.0).astype(BF16)
    tiles = half // QT

    def update(pieces, masked=False):
        count = len(pieces) * blk

        def keys():
            return jnp.concatenate([kv_all[b, s, core] for b, s, core in pieces], axis=0)

        v_s[pl.ds(0, count), :] = keys() * keep_high + ones_low
        gate_row = jnp.concatenate(
            [
                gate_all[b, core, pl.ds(s * tiles_blk + i, 1), :]
                for b, s, core in pieces
                for i in range(tiles_blk)
            ],
            axis=1,
        )

        def score_of(t):
            score = lax.dot_general(
                q_s[pl.ds(t * QT, QT), :],
                keys(),
                (((1,), (1,)), ((), ())),
                preferred_element_type=F32,
            )
            score = score - gate_row
            if masked:
                shape = score.shape
                row_id = lax.broadcasted_iota(jnp.int32, shape, 0) + t * QT
                score = jnp.where(
                    lax.broadcasted_iota(jnp.int32, shape, 1) <= row_id, score, -jnp.inf
                )
            return score

        def add(t, score):
            rows = pl.ds(t * QT, QT)
            gt = gt_s[rows, :]
            m_old = m_s[rows, :]
            m_new = jnp.maximum(m_old, jnp.max(score, axis=1, keepdims=True) + gt)
            wide = jnp.concatenate([m_new - gt] * (count // LANES), axis=1)
            probs = jnp.exp(score - wide).astype(BF16)
            o_s[rows, :] = o_s[rows, :] * jnp.exp(m_old - m_new) + jnp.dot(
                probs, v_s[pl.ds(0, count), :], preferred_element_type=F32
            )
            m_s[rows, :] = m_new

        score = score_of(0)
        for t in range(tiles):
            following = score_of(t + 1) if t + 1 < tiles else None
            add(t, score)
            score = following

    update([(z, s, c) for s in range(subs)], masked=True)

    @pl.when(c == 1)
    def _():
        for s in range(subs):
            chunk_wait(s, own_rs.at[s])
        update([(z, s, 0) for s in range(subs)])

    def pieces_of(d, k, s):
        return [(block_of(d, k), s, core) for core in range(2)]

    def relayed(d, k, s):
        chunk_wait(s, d2d_rs.at[d, k - 1, s])

    def pair(k, s):
        @pl.when(needs(1, k, s))
        def _():
            relayed(0, k, s)
            relayed(1, k, s)
            update(pieces_of(0, k, s) + pieces_of(1, k, s))

        @pl.when(jnp.logical_and(needs(0, k, s), jnp.logical_not(needs(1, k, s))))
        def _():
            relayed(0, k, s)
            update(pieces_of(0, k, s))

    def pass_on(d, k, s):
        @pl.when(receives(d, k, s))
        def _():
            b = block_of(d, k)
            chunk_wait(s, ring_rs.at[d, k - 1, s])

            @pl.when(sends(d, k + 1, s))
            def _():
                @pl.when(sends(d, k, s))
                def _():
                    chunk_wait(s, ring_ss.at[d, s])

                for copy in chunk_copies(b, s, links[d], ring_ss.at[d, s], ring_rs.at[d, k, s]):
                    copy.start()

            @pl.when(needs(d, k, s))
            def _():
                @pl.when(jnp.logical_and(k > 1, needs(d, k - 1, s)))
                def _():
                    chunk_wait(s, d2d_ss.at[d, s])

                for copy in chunk_copies(
                    b, s, partner, d2d_ss.at[d, s], d2d_rs.at[d, k - 1, s]
                ):
                    copy.start()

    @pl.loop(1, k_up)
    def _(k):
        pass_on(0, k, 0)
        pass_on(1, k, 0)

        @pl.when(k > 1)
        def _():
            pair(k - 1, 1)

        pass_on(0, k, 1)
        pass_on(1, k, 1)
        pair(k, 0)

        @pl.when(k == 3)
        def _():
            wout_gather.relay()

        @pl.when(k == 5)
        def _():
            wout_gather.finish_links()

    for s in range(subs):
        pass_on(s, k_up, s)
    pair(k_up - 1, 1)

    @pl.when(z >= k_up)
    def _():
        for s in range(subs):
            relayed(s, k_up, s)
        update([(z - k_up, s, core) for s in range(subs) for core in range(2)])

    odd_head = lax.rem(y, 2) == 1
    few = rows_tp // 2

    for n in range(half // rows_tp):
        first = o_s[pl.ds(n * rows_tp, few), :]
        second = o_s[pl.ds(n * rows_tp + few, few), :]
        first = pltpu.roll(first, HEAD, 1) / first
        second = second / pltpu.roll(second, HEAD, 1)
        att_send[n] = jnp.where(low[:few], first, second).astype(BF16)

    head = NY * x + y
    att = []
    for s in range(subs):
        for t in range(NX * NC):
            ty = 2 * c + s
            src = att_send.at[s * NX * NC + t]
            remote = pltpu.make_async_remote_copy(
                src_ref=src,
                dst_ref=att_recv.at[head],
                send_sem=att_ss,
                recv_sem=att_rs,
                device_id=(z * NY + ty, t),
                device_id_type=MESH,
            )
            local = pltpu.make_async_copy(src, att_recv.at[head], att_rs)
            is_self = jnp.logical_and(ty == y, tp == t)

            @pl.when(jnp.logical_not(is_self))
            def _():
                remote.start()

            @pl.when(is_self)
            def _():
                local.start()

    wout_gather.finish()
    pltpu.make_async_copy(att_recv, att_recv, att_rs).wait()

    groups = NX * NC
    pairs = []
    for g in range(groups):
        even, odd = [att_recv[2 * g + n].astype(F32) for n in range(2)]
        early = jnp.where(low[:few], even, pltpu.roll(odd, HEAD, 1))
        late = jnp.where(low[:few], pltpu.roll(even, HEAD, 1), odd)
        pairs.append(jnp.concatenate([early, late], axis=0).astype(BF16))
    cols = 256

    @pl.loop(0, out_ref.shape[1] // cols)
    def _(t):
        span = pl.ds(pl.multiple_of(t * cols, cols), cols)
        acc = jnp.zeros((rows_tp, cols), F32)
        for g in range(groups):
            part = jnp.dot(
                pairs[g],
                wout[pl.ds(g * wout_rows, wout_rows), span],
                preferred_element_type=F32,
            )
            acc = acc + part.astype(BF16).astype(F32)
        out_ref[:, span] = acc.astype(BF16)

    tok_gather.drain()
    wout_gather.drain()
    for j, remote in exchanged:

        @pl.when(j != y)
        def _():
            remote.wait_send()

    @pl.when(c == 0)
    def _():
        for s in range(subs):
            chunk_wait(s, own_ss.at[s])

    @pl.loop(1, k_up + 1)
    def _(k):
        for d in range(2):
            for s in range(subs):
                more = jnp.logical_not(sends(d, k + 1, s))

                @pl.when(jnp.logical_and(sends(d, k, s), more))
                def _():
                    chunk_wait(s, ring_ss.at[d, s])

                more = jnp.logical_not(needs(d, k + 1, s))

                @pl.when(jnp.logical_and(needs(d, k, s), more))
                def _():
                    chunk_wait(s, d2d_ss.at[d, s])

    stays = owner_core == c
    pieces = att_send.shape[0]

    @pl.when(stays)
    def _():
        sent = att_send.at[pl.ds(0, pieces - 1)]
        pltpu.make_async_copy(sent, sent, att_ss).wait()

    @pl.when(jnp.logical_not(stays))
    def _():
        pltpu.make_async_copy(att_send, att_send, att_ss).wait()


def on_device(
    nz,
    tokens,
    query_weight,
    key_weight,
    value_weight,
    query_gain,
    key_gain,
    log_gate_total,
    output_weight,
):
    rows_tp, depth = tokens.shape
    width = query_weight.shape[1]
    blk, heads = log_gate_total.shape
    half = 2 * blk
    k_up = nz // 2
    dma = pltpu.SemaphoreType.DMA
    any_spec = pl.BlockSpec(memory_space=pl.ANY)
    vmem_spec = pl.BlockSpec(memory_space=pltpu.VMEM)
    return pl.pallas_call(
        functools.partial(kernel, nz),
        out_shape=jax.ShapeDtypeStruct((rows_tp, output_weight.shape[1]), BF16),
        in_specs=[any_spec] * 8,
        out_specs=vmem_spec,
        scratch_shapes=[
            pltpu.VMEM((blk, depth), BF16),
            pltpu.VMEM((depth, 3 * width), BF16),
            pltpu.VMEM((NX * NC * output_weight.shape[0], output_weight.shape[1]), BF16),
            pltpu.VMEM((blk, 2 * width), F32),
            pltpu.VMEM((2, blk, LANES), BF16),
            pltpu.VMEM((2, blk // 2, LANES), BF16),
            pltpu.VMEM((2, 1, HEAD), F32),
            pltpu.VMEM((heads, blk), F32),
            pltpu.VMEM((2, 8, LANES), F32),
            pltpu.VMEM((2, blk // 2, LANES), BF16),
            pltpu.VMEM((2, 8, LANES), F32),
            pltpu.VMEM((nz, 2, 2, blk, LANES), BF16),
            pltpu.VMEM((nz, 2, 8, LANES), F32),
            pltpu.VMEM((half, LANES), BF16),
            pltpu.VMEM((half, LANES), F32),
            pltpu.VMEM((half, LANES), F32),
            pltpu.VMEM((half, LANES), F32),
            pltpu.VMEM((2 * half, LANES), BF16),
            pltpu.VMEM((2 * NX * NC, rows_tp // 2, LANES), BF16),
            pltpu.VMEM((NX * NY, rows_tp // 2, LANES), BF16),
            dma((8,)),
            dma,
            dma((13,)),
            dma,
            dma((13,)),
            dma((3, 2)),
            dma((3, 2)),
            dma((2, 2)),
            dma((2, k_up, 2)),
            dma((2, 2)),
            dma((2, k_up, 2)),
            dma((2,)),
            dma((2,)),
            dma,
            dma,
        ],
        compiler_params=pltpu.CompilerParams(
            collective_id=0, has_side_effects=True, vmem_limit_bytes=60 * 1024 * 1024
        ),
    )(
        tokens,
        query_weight,
        key_weight,
        value_weight,
        query_gain[None, :],
        key_gain[None, :],
        log_gate_total.T,
        output_weight,
    )


def solution(mesh):
    placed = (
        P(("sp", "tp"), None),
        P(None, "tp"),
        P(None, "tp"),
        P(None, "tp"),
        P(),
        P(),
        P("sp", "tp"),
        P("tp", None),
    )
    nz = mesh.shape["sp"] // NY
    return jax.shard_map(
        functools.partial(on_device, nz),
        mesh=mesh,
        in_specs=placed,
        out_specs=P(("sp", "tp"), None),
        check_vma=False,
    )
```

```python
import functools

import jax
import jax.numpy as jnp
from jax import lax
from jax.experimental import pallas as pl
from jax.experimental.pallas import tpu as pltpu
from jax.sharding import PartitionSpec as P

NORM_EPS = 1e-06
MESH = pl.DeviceIdType.MESH
F32 = jnp.float32
BF16 = jnp.bfloat16
LANES = 128
HEAD = 64
NX = 4
NY = 4
NC = 2
QT = 384


class RowGather:
    def __init__(self, buf, rows, x, c, ids, ssem, rsem):
        self.buf, self.rows, self.x, self.c = buf, rows, x, c
        self.right, self.left, self.partner = ids
        self.ssem, self.rsem = ssem, rsem
        self.half = buf.shape[1] // 2

    def piece(self, dx, core, part):
        slot = lax.rem(self.x + dx + NX, NX) * NC + core
        rows = pl.ds(pl.multiple_of(slot * self.rows, self.rows), self.rows)
        if part is None:
            return self.buf.at[rows]
        return self.buf.at[rows, pl.ds(part * self.half, self.half)]

    def copy(self, dx, core, part, index):
        device = self.right if index < 3 else self.left if index < 6 else self.partner
        piece = self.piece(dx, core, part)
        return pltpu.make_async_remote_copy(
            src_ref=piece,
            dst_ref=piece,
            send_sem=self.ssem,
            recv_sem=self.rsem.at[index],
            device_id=device,
            device_id_type=MESH,
        )

    def send(self, dx, part, index):
        self.copy(dx, self.c, part, index).start()

    def arrive(self, dx, core, part, index):
        self.copy(dx, core, part, index).wait_recv()

    def start(self):
        self.send(0, 0, 0)
        self.send(0, 1, 3)
        self.send(0, 1, 1)
        self.send(0, 0, 4)
        self.send(0, None, 6)

    def relay(self):
        self.arrive(-1, self.c, 0, 0)
        self.send(-1, 0, 2)
        self.arrive(1, self.c, 1, 3)
        self.send(1, 1, 5)
        self.send(-1, 0, 7)
        self.send(1, 1, 8)

    def relay_near(self):
        self.arrive(-1, self.c, 1, 1)
        self.send(-1, 1, 9)
        self.arrive(1, self.c, 0, 4)
        self.send(1, 0, 10)

    def relay_far(self):
        self.arrive(-2, self.c, 0, 2)
        self.send(-2, 0, 11)
        self.arrive(2, self.c, 1, 5)
        self.send(2, 1, 12)

    def finish_own(self):
        self.arrive(0, 1 - self.c, None, 6)

    def finish_near(self):
        other = 1 - self.c
        self.arrive(-1, other, 0, 7)
        self.arrive(1, other, 1, 8)
        self.arrive(-1, other, 1, 9)
        self.arrive(1, other, 0, 10)

    def finish_far(self):
        other = 1 - self.c
        self.arrive(-2, other, 0, 11)
        self.arrive(2, other, 1, 12)

    def drain(self):
        sent = self.buf.at[pl.ds(0, 7 * self.rows)]
        pltpu.make_async_copy(sent, sent, self.ssem).wait()


def kernel(
    nz,
    tokens_ref,
    wq_ref,
    wk_ref,
    wv_ref,
    qgain_ref,
    kgain_ref,
    gates_ref,
    wout_ref,
    out_ref,
    tok,
    wqkv,
    wout,
    q_raw,
    kv_send,
    q_send,
    gain_v,
    gate_v,
    gate_send,
    q_recv,
    gate_recv,
    kv_all,
    gate_all,
    q_s,
    gt_s,
    m_s,
    o_s,
    v_s,
    att_send,
    att_recv,
    acc_s,
    lsem,
    tok_ss,
    tok_rs,
    wo_ss,
    wo_rs,
    a2a_ss,
    a2a_rs,
    ring_ss,
    ring_rs,
    d2d_ss,
    d2d_rs,
    own_ss,
    own_rs,
    att_ss,
    att_rs,
):
    sp = lax.axis_index("sp")
    tp = lax.axis_index("tp")
    z, y = lax.div(sp, NY), lax.rem(sp, NY)
    x, c = lax.div(tp, NC), lax.rem(tp, NC)

    def device(dz, dy, dx, dc):
        return (dz * NY + dy, dx * NC + dc)

    right = device(z, y, lax.rem(x + 1, NX), c)
    left = device(z, y, lax.rem(x + NX - 1, NX), c)
    partner = device(z, y, x, 1 - c)
    up = device(lax.rem(z + 1, nz), y, x, c)
    down = device(lax.rem(z + nz - 1, nz), y, x, c)
    owner_core = lax.div(y, 2)

    rows_tp = tokens_ref.shape[0]
    blk = rows_tp * NX * NC
    half = 2 * blk
    width = wq_ref.shape[1]

    own_rows = pl.ds(pl.multiple_of(tp * rows_tp, rows_tp), rows_tp)
    wout_rows = wout_ref.shape[0]
    load_tok = pltpu.make_async_copy(tokens_ref, tok.at[own_rows], lsem.at[0])
    load_tok.start()
    loads = []
    for i, w_ref in enumerate((wq_ref, wk_ref, wv_ref)):
        loads.append(
            pltpu.make_async_copy(w_ref, wqkv.at[:, pl.ds(i * width, width)], lsem.at[1 + i])
        )
    load_wout = pltpu.make_async_copy(
        wout_ref,
        wout.at[pl.ds(pl.multiple_of(tp * wout_rows, wout_rows), wout_rows)],
        lsem.at[4],
    )
    for load in loads:
        load.start()
    load_wout.start()
    smalls = []
    for i, (src, dst) in enumerate(
        ((qgain_ref, gain_v.at[0]), (kgain_ref, gain_v.at[1]), (gates_ref, gate_v))
    ):
        smalls.append(pltpu.make_async_copy(src, dst, lsem.at[5 + i]))
        smalls[-1].start()

    barrier = pltpu.get_barrier_semaphore()
    for neighbour in (right, left, partner, up, down):
        pl.semaphore_signal(barrier, inc=1, device_id=neighbour, device_id_type=MESH)
    for i in range(2):
        j = 2 * c + i

        @pl.when(j != y)
        def _():
            pl.semaphore_signal(
                barrier, inc=1, device_id=device(z, j, x, owner_core), device_id_type=MESH
            )

    @pl.when(owner_core == c)
    def _():
        pl.semaphore_wait(barrier, 6)

    @pl.when(owner_core != c)
    def _():
        pl.semaphore_wait(barrier, 7)

    load_tok.wait()
    tok_gather = RowGather(tok, rows_tp, x, c, (right, left, partner), tok_ss, tok_rs)
    tok_gather.start()
    par = lax.rem(y, 2)
    tiles_blk = blk // LANES

    for small in smalls:
        small.wait()
    sublane = lax.broadcasted_iota(jnp.int32, (8, LANES), 0)
    for i in range(2):
        tile = jnp.zeros((8, LANES), F32)
        for t in range(tiles_blk):
            row = jnp.broadcast_to(gate_v[i : i + 1, t * LANES : (t + 1) * LANES], (8, LANES))
            tile = jnp.where(sublane == par * tiles_blk + t, row, tile)
        gate_send[i] = tile

    def exchange(n, i, src, dst):
        j = 2 * c + i
        remote = pltpu.make_async_remote_copy(
            src_ref=src,
            dst_ref=dst,
            send_sem=a2a_ss.at[n, i],
            recv_sem=a2a_rs.at[n, par],
            device_id=device(z, j, x, owner_core),
            device_id_type=MESH,
        )

        @pl.when(j != y)
        def _():
            remote.start()

        @pl.when(j == y)
        def _():
            pltpu.make_async_copy(src, dst, a2a_rs.at[n, par]).start()


    def received(n, s, dst):
        pltpu.make_async_copy(dst, dst, a2a_rs.at[n, s]).wait()

    for i in range(2):
        exchange(2, i, gate_send.at[i], gate_recv.at[par])

    lane = lax.broadcasted_iota(jnp.int32, (LANES, LANES), 1)
    low = lane < HEAD
    qgain, kgain = [jnp.concatenate([gain_v[i], gain_v[i]], axis=1) for i in range(2)]
    chip_rows = NC * rows_tp

    def head_norm(raw_part, gain):
        low_part = low[: raw_part.shape[0]]
        square = raw_part * raw_part
        lo = jnp.sum(jnp.where(low_part, square, 0.0), axis=1, keepdims=True) * (1.0 / HEAD)
        hi = jnp.sum(jnp.where(low_part, 0.0, square), axis=1, keepdims=True) * (1.0 / HEAD)
        inverse = jnp.where(low_part, lax.rsqrt(lo + NORM_EPS), lax.rsqrt(hi + NORM_EPS))
        return raw_part * inverse * gain

    def rows_of(dx):
        slot = lax.rem(x + dx + NX, NX)
        return pl.ds(pl.multiple_of(slot * chip_rows, chip_rows), chip_rows)

    def project_keys(dx):
        rows = rows_of(dx)
        low_part = low[:chip_rows]
        raw = jnp.dot(tok[rows, :], wqkv[:, width : 3 * width], preferred_element_type=F32)
        k_part = head_norm(raw[:, 0:width], kgain)
        v_part = raw[:, width : 2 * width]
        k_roll = pltpu.roll(k_part, HEAD, 1)
        v_roll = pltpu.roll(v_part, HEAD, 1)
        kv_send[0, rows, :] = jnp.where(low_part, k_part, v_roll).astype(BF16)
        kv_send[1, rows, :] = jnp.where(low_part, k_roll, v_part).astype(BF16)
        for i in range(2):
            exchange(0, i, kv_send.at[i, rows], kv_all.at[z, par, owner_core, rows])

    def project_queries(dx):
        rows = rows_of(dx)
        raw = jnp.dot(tok[rows, :], wqkv[:, 0:width], preferred_element_type=F32)
        q_raw[rows, :] = head_norm(raw, qgain) * (HEAD**-0.5)

    for load in loads:
        load.wait()
    tok_gather.finish_own()
    project_keys(0)
    tok_gather.relay()
    project_queries(0)
    tok_gather.relay_near()
    tok_gather.finish_near()
    project_keys(1)
    project_keys(-1)
    tok_gather.relay_far()
    load_wout.wait()
    wout_gather = RowGather(wout, wout_rows, x, c, (right, left, partner), wo_ss, wo_rs)
    wout_gather.start()
    project_queries(1)
    tok_gather.finish_far()
    project_keys(2)

    project_queries(-1)
    project_queries(2)
    pack = blk // 2
    step = 64
    for t in range(pack // step):
        first = q_raw[pl.ds(t * step, step), :]
        second = q_raw[pl.ds(pack + t * step, step), :]
        rows = pl.ds(t * step, step)
        q_send[0, rows, :] = jnp.where(low[:step], first, pltpu.roll(second, HEAD, 1)).astype(BF16)
        q_send[1, rows, :] = jnp.where(low[:step], pltpu.roll(first, HEAD, 1), second).astype(BF16)
    for i in range(2):
        exchange(1, i, q_send.at[i], q_recv.at[par])

    subs = 2

    def chunk_copies(b, s, target, send_sem, recv_sem):
        pieces = (kv_all.at[b, s, c], gate_all.at[b, c])
        return [
            pltpu.make_async_remote_copy(
                src_ref=piece,
                dst_ref=piece,
                send_sem=send_sem,
                recv_sem=recv_sem,
                device_id=target,
                device_id_type=MESH,
            )
            for piece in (pieces if s == 0 else pieces[:1])
        ]

    def chunk_wait(s, sem):
        gate_rows = 8 * LANES * 4 // (LANES * 2)
        sized = v_s.at[pl.ds(0, blk + gate_rows if s == 0 else blk)]
        pltpu.make_async_copy(sized, sized, sem).wait()

    k_up = nz // 2
    links = (up, down)

    def block_of(d, k):
        return z - k if d == 0 else lax.rem(z + k, nz)

    def whole(d, k, s):
        return k <= (k_up if s == d else k_up - 1)

    def highest(s):
        return k_up - 1 if s == 1 else k_up - 2

    def receives(d, k, s):
        block = block_of(d, k)
        return jnp.logical_and(block >= 0 if d == 0 else block <= highest(s), whole(d, k, s))

    def sends(d, k, s):
        if d == 0:
            there = jnp.logical_and(z - k + 1 >= 0, z <= nz - 2)
        else:
            there = lax.rem(z + k - 1, nz) <= highest(s)
        return jnp.logical_and(there, whole(d, k, s))

    def needs(d, k, s):
        if d == 0:
            return receives(0, k, s)
        return jnp.logical_and(receives(1, k, s), block_of(1, k) < z)

    for s in range(subs):
        received(2, s, gate_recv.at[s])
    gate_all[z, c] = gate_recv[0] + gate_recv[1]
    for s in range(subs):
        received(0, s, kv_all.at[z, s, c])
        for d in range(2):

            @pl.when(sends(d, 1, s))
            def _():
                for copy in chunk_copies(z, s, links[d], ring_ss.at[d, s], ring_rs.at[d, 0, s]):
                    copy.start()

    @pl.when(c == 0)
    def _():
        for s in range(subs):
            for copy in chunk_copies(z, s, partner, own_ss.at[s], own_rs.at[s]):
                copy.start()

    gate_t = jnp.transpose(gate_all[z, c])
    for t in range(2 * tiles_blk):
        column = gate_t[:, t : t + 1]
        gt_s[pl.ds(t * LANES, LANES), :] = jnp.broadcast_to(column, (LANES, LANES))
    m_s[...] = jnp.full(m_s.shape, -1e30, F32)
    o_s[...] = jnp.zeros(o_s.shape, F32)
    for s in range(subs):
        received(1, s, q_recv.at[s])
        for t in range(pack // step):
            packed = q_recv[s, pl.ds(t * step, step), :].astype(F32)
            second = pltpu.roll(packed, HEAD, 1)
            for n, rows in enumerate((packed, second)):
                first_row = s * blk + n * pack + t * step
                q_s[pl.ds(first_row, step), :] = jnp.where(low[:step], rows, 0.0).astype(BF16)

    lane_row = lax.broadcasted_iota(jnp.int32, (1, LANES), 1)
    ones_low = jnp.where(lane_row < HEAD, 1.0, 0.0).astype(BF16)
    keep_high = jnp.where(lane_row < HEAD, 0.0, 1.0).astype(BF16)
    tiles = half // QT

    def update(pieces, masked=False):
        count = len(pieces) * blk

        def keys():
            return jnp.concatenate([kv_all[b, s, core] for b, s, core in pieces], axis=0)

        v_s[pl.ds(0, count), :] = keys() * keep_high + ones_low
        gate_row = jnp.concatenate(
            [
                gate_all[b, core, pl.ds(s * tiles_blk + i, 1), :]
                for b, s, core in pieces
                for i in range(tiles_blk)
            ],
            axis=1,
        )

        def score_of(t):
            score = lax.dot_general(
                q_s[pl.ds(t * QT, QT), :],
                keys(),
                (((1,), (1,)), ((), ())),
                preferred_element_type=F32,
            )
            score = score - gate_row
            if masked:
                shape = score.shape
                row_id = lax.broadcasted_iota(jnp.int32, shape, 0) + t * QT
                score = jnp.where(
                    lax.broadcasted_iota(jnp.int32, shape, 1) <= row_id, score, -jnp.inf
                )
            return score

        def add(t, score):
            rows = pl.ds(t * QT, QT)
            gt = gt_s[rows, :]
            m_old = m_s[rows, :]
            m_new = jnp.maximum(m_old, jnp.max(score, axis=1, keepdims=True) + gt)
            wide = jnp.concatenate([m_new - gt] * (count // LANES), axis=1)
            probs = jnp.exp(score - wide).astype(BF16)
            o_s[rows, :] = o_s[rows, :] * jnp.exp(m_old - m_new) + jnp.dot(
                probs, v_s[pl.ds(0, count), :], preferred_element_type=F32
            )
            m_s[rows, :] = m_new

        score = score_of(0)
        for t in range(tiles):
            following = score_of(t + 1) if t + 1 < tiles else None
            add(t, score)
            score = following

    update([(z, s, c) for s in range(subs)], masked=True)

    @pl.when(c == 1)
    def _():
        for s in range(subs):
            chunk_wait(s, own_rs.at[s])
        update([(z, s, 0) for s in range(subs)])

    def pieces_of(d, k, s):
        return [(block_of(d, k), s, core) for core in range(2)]

    def relayed(d, k, s):
        chunk_wait(s, d2d_rs.at[d, k - 1, s])

    def pair(k, s):
        @pl.when(needs(1, k, s))
        def _():
            relayed(0, k, s)
            relayed(1, k, s)
            update(pieces_of(0, k, s) + pieces_of(1, k, s))

        @pl.when(jnp.logical_and(needs(0, k, s), jnp.logical_not(needs(1, k, s))))
        def _():
            relayed(0, k, s)
            update(pieces_of(0, k, s))

    def pass_on(d, k, s):
        @pl.when(receives(d, k, s))
        def _():
            b = block_of(d, k)
            chunk_wait(s, ring_rs.at[d, k - 1, s])

            @pl.when(sends(d, k + 1, s))
            def _():
                @pl.when(sends(d, k, s))
                def _():
                    chunk_wait(s, ring_ss.at[d, s])

                for copy in chunk_copies(b, s, links[d], ring_ss.at[d, s], ring_rs.at[d, k, s]):
                    copy.start()

            @pl.when(needs(d, k, s))
            def _():
                @pl.when(jnp.logical_and(k > 1, needs(d, k - 1, s)))
                def _():
                    chunk_wait(s, d2d_ss.at[d, s])

                for copy in chunk_copies(
                    b, s, partner, d2d_ss.at[d, s], d2d_rs.at[d, k - 1, s]
                ):
                    copy.start()

    @pl.loop(1, k_up)
    def _(k):
        pass_on(0, k, 0)
        pass_on(1, k, 0)

        @pl.when(k > 1)
        def _():
            pair(k - 1, 1)

        pass_on(0, k, 1)
        pass_on(1, k, 1)
        pair(k, 0)

        @pl.when(k == 3)
        def _():
            wout_gather.relay()

        @pl.when(k == 5)
        def _():
            wout_gather.relay_near()
            wout_gather.relay_far()

    for s in range(subs):
        pass_on(s, k_up, s)
    pair(k_up - 1, 1)

    @pl.when(z >= k_up)
    def _():
        for s in range(subs):
            relayed(s, k_up, s)
        update([(z - k_up, s, core) for s in range(subs) for core in range(2)])

    odd_head = lax.rem(y, 2) == 1
    few = rows_tp // 2

    for n in range(half // rows_tp):
        first = o_s[pl.ds(n * rows_tp, few), :]
        second = o_s[pl.ds(n * rows_tp + few, few), :]
        first = pltpu.roll(first, HEAD, 1) / first
        second = second / pltpu.roll(second, HEAD, 1)
        att_send[n] = jnp.where(low[:few], first, second).astype(BF16)

    head = NY * x + y
    att = []
    for s in range(subs):
        for t in range(NX * NC):
            ty = 2 * c + s
            src = att_send.at[s * NX * NC + t]
            remote = pltpu.make_async_remote_copy(
                src_ref=src,
                dst_ref=att_recv.at[head],
                send_sem=att_ss,
                recv_sem=att_rs.at[x],
                device_id=(z * NY + ty, t),
                device_id_type=MESH,
            )
            local = pltpu.make_async_copy(src, att_recv.at[head], att_rs.at[x])
            is_self = jnp.logical_and(ty == y, tp == t)

            @pl.when(jnp.logical_not(is_self))
            def _():
                remote.start()

            @pl.when(is_self)
            def _():
                local.start()

    wout_gather.finish_own()
    wout_gather.finish_near()
    wout_gather.finish_far()
    cols = 256
    for n, dx in enumerate((0, 1, -1, 2)):
        slot = lax.rem(x + dx + NX, NX)
        heads = att_recv.at[pl.ds(slot * NY, NY)]
        pltpu.make_async_copy(heads, heads, att_rs.at[slot]).wait()
        pairs = []
        for g in range(NC):
            even, odd = [att_recv[slot * NY + 2 * g + i].astype(F32) for i in range(2)]
            early = jnp.where(low[:few], even, pltpu.roll(odd, HEAD, 1))
            late = jnp.where(low[:few], pltpu.roll(even, HEAD, 1), odd)
            pairs.append(jnp.concatenate([early, late], axis=0).astype(BF16))

        @pl.loop(0, out_ref.shape[1] // cols)
        def _(t):
            span = pl.ds(pl.multiple_of(t * cols, cols), cols)
            acc = None if n == 0 else acc_s[:, span]
            for g in range(NC):
                first = pl.multiple_of((slot * NC + g) * wout_rows, wout_rows)
                part = jnp.dot(
                    pairs[g], wout[pl.ds(first, wout_rows), span], preferred_element_type=F32
                )
                part = part.astype(BF16).astype(F32)
                acc = part if acc is None else acc + part
            if n < NX - 1:
                acc_s[:, span] = acc
            else:
                out_ref[:, span] = acc.astype(BF16)

    tok_gather.drain()
    wout_gather.drain()
    for i in range(2):

        @pl.when(2 * c + i != y)
        def _():
            for n, sent in enumerate((kv_send.at[i], q_send.at[i], gate_send.at[i])):
                pltpu.make_async_copy(sent, sent, a2a_ss.at[n, i]).wait()

    @pl.when(c == 0)
    def _():
        for s in range(subs):
            chunk_wait(s, own_ss.at[s])

    @pl.loop(1, k_up + 1)
    def _(k):
        for d in range(2):
            for s in range(subs):
                more = jnp.logical_not(sends(d, k + 1, s))

                @pl.when(jnp.logical_and(sends(d, k, s), more))
                def _():
                    chunk_wait(s, ring_ss.at[d, s])

                more = jnp.logical_not(needs(d, k + 1, s))

                @pl.when(jnp.logical_and(needs(d, k, s), more))
                def _():
                    chunk_wait(s, d2d_ss.at[d, s])

    stays = owner_core == c
    pieces = att_send.shape[0]

    @pl.when(stays)
    def _():
        sent = att_send.at[pl.ds(0, pieces - 1)]
        pltpu.make_async_copy(sent, sent, att_ss).wait()

    @pl.when(jnp.logical_not(stays))
    def _():
        pltpu.make_async_copy(att_send, att_send, att_ss).wait()


def on_device(
    nz,
    tokens,
    query_weight,
    key_weight,
    value_weight,
    query_gain,
    key_gain,
    log_gate_total,
    output_weight,
):
    rows_tp, depth = tokens.shape
    width = query_weight.shape[1]
    blk, heads = log_gate_total.shape
    half = 2 * blk
    k_up = nz // 2
    dma = pltpu.SemaphoreType.DMA
    any_spec = pl.BlockSpec(memory_space=pl.ANY)
    vmem_spec = pl.BlockSpec(memory_space=pltpu.VMEM)
    return pl.pallas_call(
        functools.partial(kernel, nz),
        out_shape=pltpu.VMEM((rows_tp, output_weight.shape[1]), BF16),
        in_specs=[any_spec] * 8,
        out_specs=vmem_spec,
        scratch_shapes=[
            pltpu.VMEM((blk, depth), BF16),
            pltpu.VMEM((depth, 3 * width), BF16),
            pltpu.VMEM((NX * NC * output_weight.shape[0], output_weight.shape[1]), BF16),
            pltpu.VMEM((blk, width), F32),
            pltpu.VMEM((2, blk, LANES), BF16),
            pltpu.VMEM((2, blk // 2, LANES), BF16),
            pltpu.VMEM((2, 1, HEAD), F32),
            pltpu.VMEM((heads, blk), F32),
            pltpu.VMEM((2, 8, LANES), F32),
            pltpu.VMEM((2, blk // 2, LANES), BF16),
            pltpu.VMEM((2, 8, LANES), F32),
            pltpu.VMEM((nz, 2, 2, blk, LANES), BF16),
            pltpu.VMEM((nz, 2, 8, LANES), F32),
            pltpu.VMEM((half, LANES), BF16),
            pltpu.VMEM((half, LANES), F32),
            pltpu.VMEM((half, LANES), F32),
            pltpu.VMEM((half, LANES), F32),
            pltpu.VMEM((2 * half, LANES), BF16),
            pltpu.VMEM((2 * NX * NC, rows_tp // 2, LANES), BF16),
            pltpu.VMEM((NX * NY, rows_tp // 2, LANES), BF16),
            pltpu.VMEM((rows_tp, output_weight.shape[1]), F32),
            dma((8,)),
            dma,
            dma((13,)),
            dma,
            dma((13,)),
            dma((3, 2)),
            dma((3, 2)),
            dma((2, 2)),
            dma((2, k_up, 2)),
            dma((2, 2)),
            dma((2, k_up, 2)),
            dma((2,)),
            dma((2,)),
            dma,
            dma((NX,)),
        ],
        compiler_params=pltpu.CompilerParams(
            collective_id=0, has_side_effects=True, vmem_limit_bytes=60 * 1024 * 1024
        ),
    )(
        tokens,
        query_weight,
        key_weight,
        value_weight,
        query_gain[None, :],
        key_gain[None, :],
        log_gate_total.T,
        output_weight,
    )


def solution(mesh):
    placed = (
        P(("sp", "tp"), None),
        P(None, "tp"),
        P(None, "tp"),
        P(None, "tp"),
        P(),
        P(),
        P("sp", "tp"),
        P("tp", None),
    )
    nz = mesh.shape["sp"] // NY
    return jax.shard_map(
        functools.partial(on_device, nz),
        mesh=mesh,
        in_specs=placed,
        out_specs=P(("sp", "tp"), None),
        check_vma=False,
    )
```

```python
import functools

import jax
import jax.numpy as jnp
from jax import lax
from jax.experimental import pallas as pl
from jax.experimental.pallas import tpu as pltpu
from jax.sharding import PartitionSpec as P

NORM_EPS = 1e-06
MESH = pl.DeviceIdType.MESH
F32 = jnp.float32
BF16 = jnp.bfloat16
LANES = 128
HEAD = 64
NX = 4
NY = 4
NC = 2
QT = 384


class RowGather:
    def __init__(self, buf, rows, x, c, ids, ssem, rsem):
        self.buf, self.rows, self.x, self.c = buf, rows, x, c
        self.right, self.left, self.partner = ids
        self.ssem, self.rsem = ssem, rsem
        self.half = buf.shape[1] // 2

    def piece(self, dx, core, part):
        slot = lax.rem(self.x + dx + NX, NX) * NC + core
        rows = pl.ds(pl.multiple_of(slot * self.rows, self.rows), self.rows)
        if part is None:
            return self.buf.at[rows]
        return self.buf.at[rows, pl.ds(part * self.half, self.half)]

    def copy(self, dx, core, part, index):
        device = self.right if index < 3 else self.left if index < 6 else self.partner
        piece = self.piece(dx, core, part)
        return pltpu.make_async_remote_copy(
            src_ref=piece,
            dst_ref=piece,
            send_sem=self.ssem,
            recv_sem=self.rsem.at[index],
            device_id=device,
            device_id_type=MESH,
        )

    def send(self, dx, part, index):
        self.copy(dx, self.c, part, index).start()

    def arrive(self, dx, core, part, index):
        self.copy(dx, core, part, index).wait_recv()

    def start(self):
        self.send(0, 0, 0)
        self.send(0, 1, 3)
        self.send(0, 1, 1)
        self.send(0, 0, 4)
        self.send(0, None, 6)

    def relay(self):
        self.arrive(-1, self.c, 0, 0)
        self.send(-1, 0, 2)
        self.arrive(1, self.c, 1, 3)
        self.send(1, 1, 5)
        self.send(-1, 0, 7)
        self.send(1, 1, 8)

    def relay_near(self):
        self.arrive(-1, self.c, 1, 1)
        self.send(-1, 1, 9)
        self.arrive(1, self.c, 0, 4)
        self.send(1, 0, 10)

    def relay_far(self):
        self.arrive(-2, self.c, 0, 2)
        self.send(-2, 0, 11)
        self.arrive(2, self.c, 1, 5)
        self.send(2, 1, 12)

    def finish_own(self):
        self.arrive(0, 1 - self.c, None, 6)

    def finish_near(self):
        other = 1 - self.c
        self.arrive(-1, other, 0, 7)
        self.arrive(1, other, 1, 8)
        self.arrive(-1, other, 1, 9)
        self.arrive(1, other, 0, 10)

    def finish_far(self):
        other = 1 - self.c
        self.arrive(-2, other, 0, 11)
        self.arrive(2, other, 1, 12)

    def drain(self):
        sent = self.buf.at[pl.ds(0, 7 * self.rows)]
        pltpu.make_async_copy(sent, sent, self.ssem).wait()


def kernel(
    nz,
    tokens_ref,
    wq_ref,
    wk_ref,
    wv_ref,
    qgain_ref,
    kgain_ref,
    gates_ref,
    wout_ref,
    out_ref,
    tok,
    wqkv,
    wout,
    q_raw,
    kv_send,
    q_send,
    gain_v,
    gate_v,
    gate_send,
    q_recv,
    gate_recv,
    kv_all,
    gate_all,
    q_s,
    gt_s,
    m_s,
    o_s,
    v_s,
    att_send,
    att_recv,
    acc_s,
    lsem,
    tok_ss,
    tok_rs,
    wo_ss,
    wo_rs,
    a2a_ss,
    a2a_rs,
    ring_ss,
    ring_rs,
    d2d_ss,
    d2d_rs,
    own_ss,
    own_rs,
    att_ss,
    att_rs,
):
    sp = lax.axis_index("sp")
    tp = lax.axis_index("tp")
    z, y = lax.div(sp, NY), lax.rem(sp, NY)
    x, c = lax.div(tp, NC), lax.rem(tp, NC)

    def device(dz, dy, dx, dc):
        return (dz * NY + dy, dx * NC + dc)

    right = device(z, y, lax.rem(x + 1, NX), c)
    left = device(z, y, lax.rem(x + NX - 1, NX), c)
    partner = device(z, y, x, 1 - c)
    up = device(lax.rem(z + 1, nz), y, x, c)
    down = device(lax.rem(z + nz - 1, nz), y, x, c)
    owner_core = lax.div(y, 2)

    rows_tp = tokens_ref.shape[0]
    blk = rows_tp * NX * NC
    half = 2 * blk
    width = wq_ref.shape[1]

    own_rows = pl.ds(pl.multiple_of(tp * rows_tp, rows_tp), rows_tp)
    wout_rows = wout_ref.shape[0]
    load_tok = pltpu.make_async_copy(tokens_ref, tok.at[own_rows], lsem.at[0])
    load_tok.start()
    loads = []
    for i, w_ref in enumerate((wq_ref, wk_ref, wv_ref)):
        loads.append(
            pltpu.make_async_copy(w_ref, wqkv.at[:, pl.ds(i * width, width)], lsem.at[1 + i])
        )
    load_wout = pltpu.make_async_copy(
        wout_ref,
        wout.at[pl.ds(pl.multiple_of(tp * wout_rows, wout_rows), wout_rows)],
        lsem.at[4],
    )
    for load in loads:
        load.start()
    load_wout.start()
    smalls = []
    for i, (src, dst) in enumerate(
        ((qgain_ref, gain_v.at[0]), (kgain_ref, gain_v.at[1]), (gates_ref, gate_v))
    ):
        smalls.append(pltpu.make_async_copy(src, dst, lsem.at[5 + i]))
        smalls[-1].start()

    barrier = pltpu.get_barrier_semaphore()
    for neighbour in (right, left, partner, up, down):
        pl.semaphore_signal(barrier, inc=1, device_id=neighbour, device_id_type=MESH)
    for i in range(2):
        j = 2 * c + i

        @pl.when(j != y)
        def _():
            pl.semaphore_signal(
                barrier, inc=1, device_id=device(z, j, x, owner_core), device_id_type=MESH
            )

    @pl.when(owner_core == c)
    def _():
        pl.semaphore_wait(barrier, 6)

    @pl.when(owner_core != c)
    def _():
        pl.semaphore_wait(barrier, 7)

    load_tok.wait()
    tok_gather = RowGather(tok, rows_tp, x, c, (right, left, partner), tok_ss, tok_rs)
    tok_gather.start()
    par = lax.rem(y, 2)
    tiles_blk = blk // LANES

    chip_rows = NC * rows_tp
    part_rows = blk // 2
    for small in smalls:
        small.wait()
    sublane = lax.broadcasted_iota(jnp.int32, (8, LANES), 0)
    wide_lane = lax.broadcasted_iota(jnp.int32, (8, half), 1)
    for i in range(2):
        line = jnp.broadcast_to(gate_v[i : i + 1, :], (8, blk))
        turned = line
        for n in range(1, NX):
            turned = jnp.where(x == n, pltpu.roll(line, blk - n * chip_rows, 1), turned)
        line = jnp.concatenate([turned, jnp.zeros((8, half - blk), F32)], axis=1)
        moved = pltpu.roll(line, part_rows, 1)
        first = jnp.where(wide_lane < part_rows, line, 0.0)
        second = jnp.where(wide_lane >= blk, moved, 0.0)
        line = first + second
        line = jnp.where(par == 0, line, pltpu.roll(line, part_rows, 1))
        tile = jnp.zeros((8, LANES), F32)
        for t in range(2 * tiles_blk):
            tile = jnp.where(sublane == t, line[:, t * LANES : (t + 1) * LANES], tile)
        gate_send[i] = tile

    def exchange(n, kind, i, src, dst):
        j = 2 * c + i
        remote = pltpu.make_async_remote_copy(
            src_ref=src,
            dst_ref=dst,
            send_sem=a2a_ss.at[kind, i],
            recv_sem=a2a_rs.at[n, par],
            device_id=device(z, j, x, owner_core),
            device_id_type=MESH,
        )

        @pl.when(j != y)
        def _():
            remote.start()

        @pl.when(j == y)
        def _():
            pltpu.make_async_copy(src, dst, a2a_rs.at[n, par]).start()

    def received(n, s, dst):
        pltpu.make_async_copy(dst, dst, a2a_rs.at[n, s]).wait()

    for i in range(2):
        exchange(3, 2, i, gate_send.at[i], gate_recv.at[par])

    lane = lax.broadcasted_iota(jnp.int32, (LANES, LANES), 1)
    low = lane < HEAD
    qgain, kgain = [jnp.concatenate([gain_v[i], gain_v[i]], axis=1) for i in range(2)]
    def head_norm(raw_part, gain):
        low_part = low[: raw_part.shape[0]]
        square = raw_part * raw_part
        lo = jnp.sum(jnp.where(low_part, square, 0.0), axis=1, keepdims=True) * (1.0 / HEAD)
        hi = jnp.sum(jnp.where(low_part, 0.0, square), axis=1, keepdims=True) * (1.0 / HEAD)
        inverse = jnp.where(low_part, lax.rsqrt(lo + NORM_EPS), lax.rsqrt(hi + NORM_EPS))
        return raw_part * inverse * gain

    def rows_of(dx):
        slot = lax.rem(x + dx + NX, NX)
        return pl.ds(pl.multiple_of(slot * chip_rows, chip_rows), chip_rows)

    def project_keys(dx):
        place = dx % NX
        kept = pl.ds(place * chip_rows, chip_rows)
        low_part = low[:chip_rows]
        raw = jnp.dot(tok[rows_of(dx), :], wqkv[:, width : 3 * width], preferred_element_type=F32)
        k_part = head_norm(raw[:, 0:width], kgain)
        v_part = raw[:, width : 2 * width]
        k_roll = pltpu.roll(k_part, HEAD, 1)
        v_roll = pltpu.roll(v_part, HEAD, 1)
        kv_send[0, kept, :] = jnp.where(low_part, k_part, v_roll).astype(BF16)
        kv_send[1, kept, :] = jnp.where(low_part, k_roll, v_part).astype(BF16)
        chunk = place // 2
        first = pl.multiple_of(par * part_rows + (place % 2) * chip_rows, chip_rows)
        there = kv_all.at[z, chunk, owner_core, pl.ds(first, chip_rows)]
        for i in range(2):
            exchange(chunk, 0, i, kv_send.at[i, kept], there)

    def project_queries(dx):
        raw = jnp.dot(tok[rows_of(dx), :], wqkv[:, 0:width], preferred_element_type=F32)
        kept = pl.ds((dx % NX) * chip_rows, chip_rows)
        q_raw[kept, :] = head_norm(raw, qgain) * (HEAD**-0.5)

    for load in loads:
        load.wait()
    tok_gather.finish_own()
    project_keys(0)
    tok_gather.relay()
    project_queries(0)
    tok_gather.relay_near()
    tok_gather.finish_near()
    project_keys(1)
    project_keys(-1)
    tok_gather.relay_far()
    load_wout.wait()
    wout_gather = RowGather(wout, wout_rows, x, c, (right, left, partner), wo_ss, wo_rs)
    wout_gather.start()
    project_queries(1)
    tok_gather.finish_far()
    project_keys(2)

    subs = 2

    def chunk_copies(b, s, target, send_sem, recv_sem):
        pieces = (kv_all.at[b, s, c], gate_all.at[b, c])
        return [
            pltpu.make_async_remote_copy(
                src_ref=piece,
                dst_ref=piece,
                send_sem=send_sem,
                recv_sem=recv_sem,
                device_id=target,
                device_id_type=MESH,
            )
            for piece in (pieces if s == 0 else pieces[:1])
        ]

    def chunk_wait(s, sem):
        gate_rows = 8 * LANES * 4 // (LANES * 2)
        sized = v_s.at[pl.ds(0, blk + gate_rows if s == 0 else blk)]
        pltpu.make_async_copy(sized, sized, sem).wait()

    k_up = nz // 2
    links = (up, down)

    def block_of(d, k):
        return z - k if d == 0 else lax.rem(z + k, nz)

    def whole(d, k, s):
        return k <= (k_up if s == d else k_up - 1)

    def highest(s):
        return k_up - 1 if s == 1 else k_up - 2

    def receives(d, k, s):
        block = block_of(d, k)
        return jnp.logical_and(block >= 0 if d == 0 else block <= highest(s), whole(d, k, s))

    def sends(d, k, s):
        if d == 0:
            there = jnp.logical_and(z - k + 1 >= 0, z <= nz - 2)
        else:
            there = lax.rem(z + k - 1, nz) <= highest(s)
        return jnp.logical_and(there, whole(d, k, s))

    def needs(d, k, s):
        if d == 0:
            return receives(0, k, s)
        return jnp.logical_and(receives(1, k, s), block_of(1, k) < z)

    for s in range(subs):
        received(3, s, gate_recv.at[s])
    gate_all[z, c] = gate_recv[0] + gate_recv[1]
    def own_to_ring(s):
        for n in range(2):
            received(s, n, kv_all.at[z, s, c, pl.ds(n * part_rows, part_rows)])
        for d in range(2):

            @pl.when(sends(d, 1, s))
            def _():
                for copy in chunk_copies(z, s, links[d], ring_ss.at[d, s], ring_rs.at[d, 0, s]):
                    copy.start()

    own_to_ring(0)

    project_queries(-1)
    project_queries(2)
    pack = blk // 2
    step = 64
    for t in range(pack // step):
        first = q_raw[pl.ds(t * step, step), :]
        second = q_raw[pl.ds(pack + t * step, step), :]
        rows = pl.ds(t * step, step)
        q_send[0, rows, :] = jnp.where(low[:step], first, pltpu.roll(second, HEAD, 1)).astype(BF16)
        q_send[1, rows, :] = jnp.where(low[:step], pltpu.roll(first, HEAD, 1), second).astype(BF16)
    for i in range(2):
        exchange(2, 1, i, q_send.at[i], q_recv.at[par])

    own_to_ring(1)

    @pl.when(c == 0)
    def _():
        for s in range(subs):
            for copy in chunk_copies(z, s, partner, own_ss.at[s], own_rs.at[s]):
                copy.start()

    gate_t = jnp.transpose(gate_all[z, c])
    for t in range(2 * tiles_blk):
        column = gate_t[:, t : t + 1]
        gt_s[pl.ds(t * LANES, LANES), :] = jnp.broadcast_to(column, (LANES, LANES))
    m_s[...] = jnp.full(m_s.shape, -1e30, F32)
    o_s[...] = jnp.zeros(o_s.shape, F32)
    for s in range(subs):
        received(2, s, q_recv.at[s])
        for t in range(pack // step):
            packed = q_recv[s, pl.ds(t * step, step), :].astype(F32)
            second = pltpu.roll(packed, HEAD, 1)
            for n, rows in enumerate((packed, second)):
                first_row = n * blk + s * part_rows + t * step
                q_s[pl.ds(first_row, step), :] = jnp.where(low[:step], rows, 0.0).astype(BF16)

    lane_row = lax.broadcasted_iota(jnp.int32, (1, LANES), 1)
    ones_low = jnp.where(lane_row < HEAD, 1.0, 0.0).astype(BF16)
    keep_high = jnp.where(lane_row < HEAD, 0.0, 1.0).astype(BF16)
    tiles = half // QT

    def position(row):
        late = (row >= blk).astype(jnp.int32)
        row = row - late * blk
        odd_y = (row >= part_rows).astype(jnp.int32)
        row = row - odd_y * part_rows
        next_slot = (row >= chip_rows).astype(jnp.int32)
        row = row - next_slot * chip_rows
        slot = lax.bitwise_and(2 * late + next_slot + x, NX - 1)
        return odd_y * blk + slot * chip_rows + row

    def update(pieces, masked=False):
        count = len(pieces) * blk

        def keys():
            return jnp.concatenate([kv_all[b, s, core] for b, s, core in pieces], axis=0)

        v_s[pl.ds(0, count), :] = keys() * keep_high + ones_low
        gate_row = jnp.concatenate(
            [
                gate_all[b, core, pl.ds(s * tiles_blk + i, 1), :]
                for b, s, core in pieces
                for i in range(tiles_blk)
            ],
            axis=1,
        )

        def score_of(t):
            score = lax.dot_general(
                q_s[pl.ds(t * QT, QT), :],
                keys(),
                (((1,), (1,)), ((), ())),
                preferred_element_type=F32,
            )
            score = score - gate_row
            if masked:
                query_pos = position(lax.broadcasted_iota(jnp.int32, (QT, 1), 0) + t * QT)
                key_pos = position(lax.broadcasted_iota(jnp.int32, (1, count), 1))
                score = jnp.where(key_pos <= query_pos, score, -jnp.inf)
            return score

        def add(t, score):
            rows = pl.ds(t * QT, QT)
            gt = gt_s[rows, :]
            m_old = m_s[rows, :]
            m_new = jnp.maximum(m_old, jnp.max(score, axis=1, keepdims=True) + gt)
            wide = jnp.concatenate([m_new - gt] * (count // LANES), axis=1)
            probs = jnp.exp(score - wide).astype(BF16)
            o_s[rows, :] = o_s[rows, :] * jnp.exp(m_old - m_new) + jnp.dot(
                probs, v_s[pl.ds(0, count), :], preferred_element_type=F32
            )
            m_s[rows, :] = m_new

        score = score_of(0)
        for t in range(tiles):
            following = score_of(t + 1) if t + 1 < tiles else None
            add(t, score)
            score = following

    def pieces_of(d, k, s):
        return [(block_of(d, k), s, core) for core in range(2)]

    def relayed(d, k, s):
        chunk_wait(s, d2d_rs.at[d, k - 1, s])

    def pair(k, s):
        @pl.when(needs(1, k, s))
        def _():
            relayed(0, k, s)
            relayed(1, k, s)
            update(pieces_of(0, k, s) + pieces_of(1, k, s))

        @pl.when(jnp.logical_and(needs(0, k, s), jnp.logical_not(needs(1, k, s))))
        def _():
            relayed(0, k, s)
            update(pieces_of(0, k, s))

    def pass_on(d, k, s):
        @pl.when(receives(d, k, s))
        def _():
            b = block_of(d, k)
            chunk_wait(s, ring_rs.at[d, k - 1, s])

            @pl.when(sends(d, k + 1, s))
            def _():
                @pl.when(sends(d, k, s))
                def _():
                    chunk_wait(s, ring_ss.at[d, s])

                for copy in chunk_copies(b, s, links[d], ring_ss.at[d, s], ring_rs.at[d, k, s]):
                    copy.start()

            @pl.when(needs(d, k, s))
            def _():
                @pl.when(jnp.logical_and(k > 1, needs(d, k - 1, s)))
                def _():
                    chunk_wait(s, d2d_ss.at[d, s])

                for copy in chunk_copies(
                    b, s, partner, d2d_ss.at[d, s], d2d_rs.at[d, k - 1, s]
                ):
                    copy.start()

    pass_on(0, 1, 0)
    pass_on(1, 1, 0)
    update([(z, s, c) for s in range(subs)], masked=True)

    @pl.when(c == 1)
    def _():
        for s in range(subs):
            chunk_wait(s, own_rs.at[s])
        update([(z, s, 0) for s in range(subs)])

    @pl.loop(1, k_up)
    def _(k):
        @pl.when(k > 1)
        def _():
            pass_on(0, k, 0)
            pass_on(1, k, 0)
            pair(k - 1, 1)

        pass_on(0, k, 1)
        pass_on(1, k, 1)
        pair(k, 0)

        @pl.when(k == 3)
        def _():
            wout_gather.relay()

        @pl.when(k == 5)
        def _():
            wout_gather.relay_near()
            wout_gather.relay_far()

    for s in range(subs):
        pass_on(s, k_up, s)
    pair(k_up - 1, 1)

    @pl.when(z >= k_up)
    def _():
        for s in range(subs):
            relayed(s, k_up, s)
        update([(z - k_up, s, core) for s in range(subs) for core in range(2)])

    odd_head = lax.rem(y, 2) == 1
    few = rows_tp // 2

    for n in range(half // rows_tp):
        first = o_s[pl.ds(n * rows_tp, few), :]
        second = o_s[pl.ds(n * rows_tp + few, few), :]
        first = pltpu.roll(first, HEAD, 1) / first
        second = second / pltpu.roll(second, HEAD, 1)
        att_send[n] = jnp.where(low[:few], first, second).astype(BF16)

    head = NY * x + y
    att = []
    for place in range(NX):
        for n in range(2 * NC):
            odd_y, core = n // NC, n % NC
            ty = 2 * c + odd_y
            t = lax.rem(x + place, NX) * NC + core
            piece = (place // 2) * NX * NC + odd_y * NX + (place % 2) * NC + core
            src = att_send.at[piece]
            remote = pltpu.make_async_remote_copy(
                src_ref=src,
                dst_ref=att_recv.at[head],
                send_sem=att_ss,
                recv_sem=att_rs.at[x],
                device_id=(z * NY + ty, t),
                device_id_type=MESH,
            )
            local = pltpu.make_async_copy(src, att_recv.at[head], att_rs.at[x])
            is_self = jnp.logical_and(ty == y, tp == t)

            @pl.when(jnp.logical_not(is_self))
            def _():
                remote.start()

            @pl.when(is_self)
            def _():
                local.start()

    wout_gather.finish_own()
    wout_gather.finish_near()
    wout_gather.finish_far()
    cols = 256
    for n, dx in enumerate((0, 1, -1, 2)):
        slot = lax.rem(x + dx + NX, NX)
        heads = att_recv.at[pl.ds(slot * NY, NY)]
        pltpu.make_async_copy(heads, heads, att_rs.at[slot]).wait()
        pairs = []
        for g in range(NC):
            even, odd = [att_recv[slot * NY + 2 * g + i].astype(F32) for i in range(2)]
            early = jnp.where(low[:few], even, pltpu.roll(odd, HEAD, 1))
            late = jnp.where(low[:few], pltpu.roll(even, HEAD, 1), odd)
            pairs.append(jnp.concatenate([early, late], axis=0).astype(BF16))

        for t in range(out_ref.shape[1] // cols):
            span = pl.ds(t * cols, cols)
            acc = None if n == 0 else acc_s[:, span]
            for g in range(NC):
                first = pl.multiple_of((slot * NC + g) * wout_rows, wout_rows)
                part = jnp.dot(
                    pairs[g], wout[pl.ds(first, wout_rows), span], preferred_element_type=F32
                )
                part = part.astype(BF16).astype(F32)
                acc = part if acc is None else acc + part
            if n < NX - 1:
                acc_s[:, span] = acc
            else:
                out_ref[:, span] = acc.astype(BF16)

    tok_gather.drain()
    wout_gather.drain()
    for i in range(2):

        @pl.when(2 * c + i != y)
        def _():
            for n, sent in enumerate((kv_send.at[i], q_send.at[i], gate_send.at[i])):
                pltpu.make_async_copy(sent, sent, a2a_ss.at[n, i]).wait()

    @pl.when(c == 0)
    def _():
        for s in range(subs):
            chunk_wait(s, own_ss.at[s])

    @pl.loop(1, k_up + 1)
    def _(k):
        for d in range(2):
            for s in range(subs):
                more = jnp.logical_not(sends(d, k + 1, s))

                @pl.when(jnp.logical_and(sends(d, k, s), more))
                def _():
                    chunk_wait(s, ring_ss.at[d, s])

                more = jnp.logical_not(needs(d, k + 1, s))

                @pl.when(jnp.logical_and(needs(d, k, s), more))
                def _():
                    chunk_wait(s, d2d_ss.at[d, s])

    stays = owner_core == c
    pieces = att_send.shape[0]

    @pl.when(stays)
    def _():
        sent = att_send.at[pl.ds(0, pieces - 1)]
        pltpu.make_async_copy(sent, sent, att_ss).wait()

    @pl.when(jnp.logical_not(stays))
    def _():
        pltpu.make_async_copy(att_send, att_send, att_ss).wait()


def on_device(
    nz,
    tokens,
    query_weight,
    key_weight,
    value_weight,
    query_gain,
    key_gain,
    log_gate_total,
    output_weight,
):
    rows_tp, depth = tokens.shape
    width = query_weight.shape[1]
    blk, heads = log_gate_total.shape
    half = 2 * blk
    k_up = nz // 2
    dma = pltpu.SemaphoreType.DMA
    any_spec = pl.BlockSpec(memory_space=pl.ANY)
    vmem_spec = pl.BlockSpec(memory_space=pltpu.VMEM)
    return pl.pallas_call(
        functools.partial(kernel, nz),
        out_shape=pltpu.VMEM((rows_tp, output_weight.shape[1]), BF16),
        in_specs=[any_spec] * 8,
        out_specs=vmem_spec,
        scratch_shapes=[
            pltpu.VMEM((blk, depth), BF16),
            pltpu.VMEM((depth, 3 * width), BF16),
            pltpu.VMEM((NX * NC * output_weight.shape[0], output_weight.shape[1]), BF16),
            pltpu.VMEM((blk, width), F32),
            pltpu.VMEM((2, blk, LANES), BF16),
            pltpu.VMEM((2, blk // 2, LANES), BF16),
            pltpu.VMEM((2, 1, HEAD), F32),
            pltpu.VMEM((heads, blk), F32),
            pltpu.VMEM((2, 8, LANES), F32),
            pltpu.VMEM((2, blk // 2, LANES), BF16),
            pltpu.VMEM((2, 8, LANES), F32),
            pltpu.VMEM((nz, 2, 2, blk, LANES), BF16),
            pltpu.VMEM((nz, 2, 8, LANES), F32),
            pltpu.VMEM((half, LANES), BF16),
            pltpu.VMEM((half, LANES), F32),
            pltpu.VMEM((half, LANES), F32),
            pltpu.VMEM((half, LANES), F32),
            pltpu.VMEM((2 * half, LANES), BF16),
            pltpu.VMEM((2 * NX * NC, rows_tp // 2, LANES), BF16),
            pltpu.VMEM((NX * NY, rows_tp // 2, LANES), BF16),
            pltpu.VMEM((rows_tp, output_weight.shape[1]), F32),
            dma((8,)),
            dma,
            dma((13,)),
            dma,
            dma((13,)),
            dma((3, 2)),
            dma((4, 2)),
            dma((2, 2)),
            dma((2, k_up, 2)),
            dma((2, 2)),
            dma((2, k_up, 2)),
            dma((2,)),
            dma((2,)),
            dma,
            dma((NX,)),
        ],
        compiler_params=pltpu.CompilerParams(
            collective_id=0, has_side_effects=True, vmem_limit_bytes=60 * 1024 * 1024
        ),
    )(
        tokens,
        query_weight,
        key_weight,
        value_weight,
        query_gain[None, :],
        key_gain[None, :],
        log_gate_total.T,
        output_weight,
    )


def solution(mesh):
    placed = (
        P(("sp", "tp"), None),
        P(None, "tp"),
        P(None, "tp"),
        P(None, "tp"),
        P(),
        P(),
        P("sp", "tp"),
        P("tp", None),
    )
    nz = mesh.shape["sp"] // NY
    return jax.shard_map(
        functools.partial(on_device, nz),
        mesh=mesh,
        in_specs=placed,
        out_specs=P(("sp", "tp"), None),
        check_vma=False,
    )
```

```python
import functools

import jax
import jax.numpy as jnp
from jax import lax
from jax.experimental import pallas as pl
from jax.experimental.pallas import tpu as pltpu
from jax.sharding import PartitionSpec as P

NORM_EPS = 1e-06
MESH = pl.DeviceIdType.MESH
F32 = jnp.float32
BF16 = jnp.bfloat16
LANES = 128
HEAD = 64
NX = 4
NY = 4
NC = 2
QT = 384


class RowGather:
    def __init__(self, buf, rows, x, c, ids, ssem, rsem):
        self.buf, self.rows, self.x, self.c = buf, rows, x, c
        self.right, self.left, self.partner = ids
        self.ssem, self.rsem = ssem, rsem
        self.half = buf.shape[1] // 2

    def piece(self, dx, core, part):
        slot = lax.rem(self.x + dx + NX, NX) * NC + core
        rows = pl.ds(pl.multiple_of(slot * self.rows, self.rows), self.rows)
        if part is None:
            return self.buf.at[rows]
        return self.buf.at[rows, pl.ds(part * self.half, self.half)]

    def copy(self, dx, core, part, index):
        device = self.right if index < 3 else self.left if index < 6 else self.partner
        piece = self.piece(dx, core, part)
        return pltpu.make_async_remote_copy(
            src_ref=piece,
            dst_ref=piece,
            send_sem=self.ssem,
            recv_sem=self.rsem.at[index],
            device_id=device,
            device_id_type=MESH,
        )

    def send(self, dx, part, index):
        self.copy(dx, self.c, part, index).start()

    def arrive(self, dx, core, part, index):
        self.copy(dx, core, part, index).wait_recv()

    def start(self):
        self.send(0, 0, 0)
        self.send(0, 1, 3)
        self.send(0, 1, 1)
        self.send(0, 0, 4)
        self.send(0, None, 6)

    def relay(self):
        self.arrive(-1, self.c, 0, 0)
        self.send(-1, 0, 2)
        self.arrive(1, self.c, 1, 3)
        self.send(1, 1, 5)
        self.send(-1, 0, 7)
        self.send(1, 1, 8)

    def relay_near(self):
        self.arrive(1, self.c, 0, 4)
        self.send(1, 0, 10)
        self.arrive(-1, self.c, 1, 1)
        self.send(-1, 1, 9)

    def relay_far(self):
        self.arrive(-2, self.c, 0, 2)
        self.send(-2, 0, 11)
        self.arrive(2, self.c, 1, 5)
        self.send(2, 1, 12)

    def finish_own(self):
        self.arrive(0, 1 - self.c, None, 6)

    def finish_right(self):
        other = 1 - self.c
        self.arrive(1, other, 1, 8)
        self.arrive(1, other, 0, 10)

    def finish_left(self):
        other = 1 - self.c
        self.arrive(-1, other, 0, 7)
        self.arrive(-1, other, 1, 9)

    def finish_far(self):
        other = 1 - self.c
        self.arrive(-2, other, 0, 11)
        self.arrive(2, other, 1, 12)

    def drain(self):
        sent = self.buf.at[pl.ds(0, 7 * self.rows)]
        pltpu.make_async_copy(sent, sent, self.ssem).wait()


def kernel(
    nz,
    tokens_ref,
    wq_ref,
    wk_ref,
    wv_ref,
    qgain_ref,
    kgain_ref,
    gates_ref,
    wout_ref,
    out_ref,
    tok,
    wqkv,
    wout,
    q_raw,
    kv_send,
    q_send,
    gain_v,
    gate_v,
    gate_send,
    q_recv,
    gate_recv,
    kv_all,
    gate_all,
    q_s,
    gt_s,
    m_s,
    o_s,
    v_s,
    att_send,
    att_recv,
    acc_s,
    lsem,
    tok_ss,
    tok_rs,
    wo_ss,
    wo_rs,
    a2a_ss,
    a2a_rs,
    ring_ss,
    ring_rs,
    d2d_ss,
    d2d_rs,
    own_ss,
    own_rs,
    att_ss,
    att_rs,
):
    sp = lax.axis_index("sp")
    tp = lax.axis_index("tp")
    z, y = lax.div(sp, NY), lax.rem(sp, NY)
    x, c = lax.div(tp, NC), lax.rem(tp, NC)

    def device(dz, dy, dx, dc):
        return (dz * NY + dy, dx * NC + dc)

    right = device(z, y, lax.rem(x + 1, NX), c)
    left = device(z, y, lax.rem(x + NX - 1, NX), c)
    partner = device(z, y, x, 1 - c)
    up = device(lax.rem(z + 1, nz), y, x, c)
    down = device(lax.rem(z + nz - 1, nz), y, x, c)
    owner_core = lax.div(y, 2)

    rows_tp = tokens_ref.shape[0]
    blk = rows_tp * NX * NC
    half = 2 * blk
    width = wq_ref.shape[1]

    own_rows = pl.ds(pl.multiple_of(tp * rows_tp, rows_tp), rows_tp)
    wout_rows = wout_ref.shape[0]
    load_tok = pltpu.make_async_copy(tokens_ref, tok.at[own_rows], lsem.at[0])
    load_tok.start()
    loads = []
    for i, w_ref in enumerate((wq_ref, wk_ref, wv_ref)):
        loads.append(
            pltpu.make_async_copy(w_ref, wqkv.at[:, pl.ds(i * width, width)], lsem.at[1 + i])
        )
    load_wout = pltpu.make_async_copy(
        wout_ref,
        wout.at[pl.ds(pl.multiple_of(tp * wout_rows, wout_rows), wout_rows)],
        lsem.at[4],
    )
    for load in loads:
        load.start()
    load_wout.start()
    smalls = []
    for i, (src, dst) in enumerate(
        ((qgain_ref, gain_v.at[0]), (kgain_ref, gain_v.at[1]), (gates_ref, gate_v))
    ):
        smalls.append(pltpu.make_async_copy(src, dst, lsem.at[5 + i]))
        smalls[-1].start()

    barrier = pltpu.get_barrier_semaphore()
    for neighbour in (right, left, partner, up, down):
        pl.semaphore_signal(barrier, inc=1, device_id=neighbour, device_id_type=MESH)
    for i in range(2):
        j = 2 * c + i

        @pl.when(j != y)
        def _():
            pl.semaphore_signal(
                barrier, inc=1, device_id=device(z, j, x, owner_core), device_id_type=MESH
            )

    @pl.when(owner_core == c)
    def _():
        pl.semaphore_wait(barrier, 6)

    @pl.when(owner_core != c)
    def _():
        pl.semaphore_wait(barrier, 7)

    load_tok.wait()
    tok_gather = RowGather(tok, rows_tp, x, c, (right, left, partner), tok_ss, tok_rs)
    tok_gather.start()
    par = lax.rem(y, 2)
    tiles_blk = blk // LANES

    chip_rows = NC * rows_tp
    part_rows = blk // 2
    for small in smalls:
        small.wait()
    sublane = lax.broadcasted_iota(jnp.int32, (8, LANES), 0)
    wide_lane = lax.broadcasted_iota(jnp.int32, (8, half), 1)
    for i in range(2):
        line = jnp.broadcast_to(gate_v[i : i + 1, :], (8, blk))
        turned = line
        for n in range(1, NX):
            turned = jnp.where(x == n, pltpu.roll(line, blk - n * chip_rows, 1), turned)
        line = jnp.concatenate([turned, jnp.zeros((8, half - blk), F32)], axis=1)
        moved = pltpu.roll(line, part_rows, 1)
        first = jnp.where(wide_lane < part_rows, line, 0.0)
        second = jnp.where(wide_lane >= blk, moved, 0.0)
        line = first + second
        line = jnp.where(par == 0, line, pltpu.roll(line, part_rows, 1))
        tile = jnp.zeros((8, LANES), F32)
        for t in range(2 * tiles_blk):
            tile = jnp.where(sublane == t, line[:, t * LANES : (t + 1) * LANES], tile)
        gate_send[i] = tile

    def exchange(n, kind, i, src, dst):
        j = 2 * c + i
        remote = pltpu.make_async_remote_copy(
            src_ref=src,
            dst_ref=dst,
            send_sem=a2a_ss.at[kind, i],
            recv_sem=a2a_rs.at[n, par],
            device_id=device(z, j, x, owner_core),
            device_id_type=MESH,
        )

        @pl.when(j != y)
        def _():
            remote.start()

        @pl.when(j == y)
        def _():
            pltpu.make_async_copy(src, dst, a2a_rs.at[n, par]).start()

    def received(n, s, dst):
        pltpu.make_async_copy(dst, dst, a2a_rs.at[n, s]).wait()

    for i in range(2):
        exchange(3, 2, i, gate_send.at[i], gate_recv.at[par])

    lane = lax.broadcasted_iota(jnp.int32, (LANES, LANES), 1)
    low = lane < HEAD
    qgain, kgain = [jnp.concatenate([gain_v[i], gain_v[i]], axis=1) for i in range(2)]
    def head_norm(raw_part, gain):
        low_part = low[: raw_part.shape[0]]
        square = raw_part * raw_part
        lo = jnp.sum(jnp.where(low_part, square, 0.0), axis=1, keepdims=True) * (1.0 / HEAD)
        hi = jnp.sum(jnp.where(low_part, 0.0, square), axis=1, keepdims=True) * (1.0 / HEAD)
        inverse = jnp.where(low_part, lax.rsqrt(lo + NORM_EPS), lax.rsqrt(hi + NORM_EPS))
        return raw_part * inverse * gain

    def rows_of(dx):
        slot = lax.rem(x + dx + NX, NX)
        return pl.ds(pl.multiple_of(slot * chip_rows, chip_rows), chip_rows)

    def project_keys(dx):
        place = dx % NX
        kept = pl.ds(place * chip_rows, chip_rows)
        low_part = low[:chip_rows]
        raw = jnp.dot(tok[rows_of(dx), :], wqkv[:, width : 3 * width], preferred_element_type=F32)
        k_part = head_norm(raw[:, 0:width], kgain)
        v_part = raw[:, width : 2 * width]
        k_roll = pltpu.roll(k_part, HEAD, 1)
        v_roll = pltpu.roll(v_part, HEAD, 1)
        kv_send[0, kept, :] = jnp.where(low_part, k_part, v_roll).astype(BF16)
        kv_send[1, kept, :] = jnp.where(low_part, k_roll, v_part).astype(BF16)
        chunk = place // 2
        first = pl.multiple_of(par * part_rows + (place % 2) * chip_rows, chip_rows)
        there = kv_all.at[z, chunk, owner_core, pl.ds(first, chip_rows)]
        for i in range(2):
            exchange(chunk, 0, i, kv_send.at[i, kept], there)

    def project_queries(dx):
        raw = jnp.dot(tok[rows_of(dx), :], wqkv[:, 0:width], preferred_element_type=F32)
        kept = pl.ds((dx % NX) * chip_rows, chip_rows)
        q_raw[kept, :] = head_norm(raw, qgain) * (HEAD**-0.5)

    for load in loads:
        load.wait()
    tok_gather.finish_own()
    project_keys(0)
    tok_gather.relay()
    project_queries(0)
    tok_gather.relay_near()
    tok_gather.finish_right()
    project_keys(1)
    tok_gather.finish_left()
    project_keys(-1)
    tok_gather.relay_far()
    load_wout.wait()
    wout_gather = RowGather(wout, wout_rows, x, c, (right, left, partner), wo_ss, wo_rs)
    wout_gather.start()
    project_queries(1)
    tok_gather.finish_far()
    project_keys(2)

    subs = 2

    def chunk_copies(b, s, target, send_sem, recv_sem):
        pieces = (kv_all.at[b, s, c], gate_all.at[b, c])
        return [
            pltpu.make_async_remote_copy(
                src_ref=piece,
                dst_ref=piece,
                send_sem=send_sem,
                recv_sem=recv_sem,
                device_id=target,
                device_id_type=MESH,
            )
            for piece in (pieces if s == 0 else pieces[:1])
        ]

    def chunk_wait(s, sem, count=1):
        gate_rows = 8 * LANES * 4 // (LANES * 2)
        sized = v_s.at[pl.ds(0, count * (blk + gate_rows if s == 0 else blk))]
        pltpu.make_async_copy(sized, sized, sem).wait()

    k_up = nz // 2
    links = (up, down)

    def block_of(d, k):
        return z - k if d == 0 else lax.rem(z + k, nz)

    def whole(d, k, s):
        return k <= (k_up if s == d else k_up - 1)

    def highest(s):
        return k_up - 1 if s == 1 else k_up - 2

    def receives(d, k, s):
        block = block_of(d, k)
        return jnp.logical_and(block >= 0 if d == 0 else block <= highest(s), whole(d, k, s))

    def sends(d, k, s):
        if d == 0:
            there = jnp.logical_and(z - k + 1 >= 0, z <= nz - 2)
        else:
            there = lax.rem(z + k - 1, nz) <= highest(s)
        return jnp.logical_and(there, whole(d, k, s))

    def needs(d, k, s):
        if d == 0:
            return receives(0, k, s)
        return jnp.logical_and(receives(1, k, s), block_of(1, k) < z)

    for s in range(subs):
        received(3, s, gate_recv.at[s])
    gate_all[z, c] = gate_recv[0] + gate_recv[1]
    def own_to_ring(s):
        for n in range(2):
            received(s, n, kv_all.at[z, s, c, pl.ds(n * part_rows, part_rows)])
        for d in range(2):

            @pl.when(sends(d, 1, s))
            def _():
                for copy in chunk_copies(z, s, links[d], ring_ss.at[d, s], ring_rs.at[d, 0, s]):
                    copy.start()

    own_to_ring(0)

    project_queries(-1)
    project_queries(2)
    pack = blk // 2
    step = 64
    for t in range(pack // step):
        first = q_raw[pl.ds(t * step, step), :]
        second = q_raw[pl.ds(pack + t * step, step), :]
        rows = pl.ds(t * step, step)
        q_send[0, rows, :] = jnp.where(low[:step], first, pltpu.roll(second, HEAD, 1)).astype(BF16)
        q_send[1, rows, :] = jnp.where(low[:step], pltpu.roll(first, HEAD, 1), second).astype(BF16)
    for i in range(2):
        exchange(2, 1, i, q_send.at[i], q_recv.at[par])

    own_to_ring(1)

    @pl.when(c == 0)
    def _():
        for s in range(subs):
            for copy in chunk_copies(z, s, partner, own_ss.at[s], own_rs.at[s]):
                copy.start()

    gate_t = jnp.transpose(gate_all[z, c])
    for t in range(2 * tiles_blk):
        column = gate_t[:, t : t + 1]
        gt_s[pl.ds(t * LANES, LANES), :] = jnp.broadcast_to(column, (LANES, LANES))
    m_s[...] = jnp.full(m_s.shape, -1e30, F32)
    o_s[...] = jnp.zeros(o_s.shape, F32)
    for s in range(subs):
        received(2, s, q_recv.at[s])
        for t in range(pack // step):
            packed = q_recv[s, pl.ds(t * step, step), :].astype(F32)
            second = pltpu.roll(packed, HEAD, 1)
            for n, rows in enumerate((packed, second)):
                first_row = n * blk + s * part_rows + t * step
                q_s[pl.ds(first_row, step), :] = jnp.where(low[:step], rows, 0.0).astype(BF16)

    lane_row = lax.broadcasted_iota(jnp.int32, (1, LANES), 1)
    ones_low = jnp.where(lane_row < HEAD, 1.0, 0.0).astype(BF16)
    keep_high = jnp.where(lane_row < HEAD, 0.0, 1.0).astype(BF16)

    def position(row):
        late = (row >= blk).astype(jnp.int32)
        row = row - late * blk
        odd_y = (row >= part_rows).astype(jnp.int32)
        row = row - odd_y * part_rows
        next_slot = (row >= chip_rows).astype(jnp.int32)
        row = row - next_slot * chip_rows
        slot = lax.bitwise_and(2 * late + next_slot + x, NX - 1)
        return odd_y * blk + slot * chip_rows + row

    def update(pieces, masked=False, order=tuple(range(half // QT)), between=None):
        count = len(pieces) * blk

        def keys():
            return jnp.concatenate([kv_all[b, s, core] for b, s, core in pieces], axis=0)

        v_s[pl.ds(0, count), :] = keys() * keep_high + ones_low
        gate_row = jnp.concatenate(
            [
                gate_all[b, core, pl.ds(s * tiles_blk + i, 1), :]
                for b, s, core in pieces
                for i in range(tiles_blk)
            ],
            axis=1,
        )

        def score_of(t):
            score = lax.dot_general(
                q_s[pl.ds(t * QT, QT), :],
                keys(),
                (((1,), (1,)), ((), ())),
                preferred_element_type=F32,
            )
            score = score - gate_row
            if masked:
                query_pos = position(lax.broadcasted_iota(jnp.int32, (QT, 1), 0) + t * QT)
                key_pos = position(lax.broadcasted_iota(jnp.int32, (1, count), 1))
                score = jnp.where(key_pos <= query_pos, score, -jnp.inf)
            return score

        def add(t, score):
            rows = pl.ds(t * QT, QT)
            gt = gt_s[rows, :]
            m_old = m_s[rows, :]
            m_new = jnp.maximum(m_old, jnp.max(score, axis=1, keepdims=True) + gt)
            wide = jnp.concatenate([m_new - gt] * (count // LANES), axis=1)
            probs = jnp.exp(score - wide).astype(BF16)
            o_s[rows, :] = o_s[rows, :] * jnp.exp(m_old - m_new) + jnp.dot(
                probs, v_s[pl.ds(0, count), :], preferred_element_type=F32
            )
            m_s[rows, :] = m_new

        score = score_of(order[0])
        for n, t in enumerate(order):
            following = score_of(order[n + 1]) if n + 1 < len(order) else None
            add(t, score)
            score = following
            if n == 0 and between is not None:
                between()

    def pieces_of(d, k, s):
        return [(block_of(d, k), s, core) for core in range(2)]

    def pair(k, s):
        @pl.when(needs(1, k, s))
        def _():
            chunk_wait(s, d2d_rs.at[k - 1, s], 2)
            update(pieces_of(0, k, s) + pieces_of(1, k, s))

        @pl.when(jnp.logical_and(needs(0, k, s), jnp.logical_not(needs(1, k, s))))
        def _():
            chunk_wait(s, d2d_rs.at[k - 1, s])
            update(pieces_of(0, k, s))

    def pass_on(d, k, s):
        @pl.when(receives(d, k, s))
        def _():
            b = block_of(d, k)
            chunk_wait(s, ring_rs.at[d, k - 1, s])

            @pl.when(sends(d, k + 1, s))
            def _():
                @pl.when(sends(d, k, s))
                def _():
                    chunk_wait(s, ring_ss.at[d, s])

                for copy in chunk_copies(b, s, links[d], ring_ss.at[d, s], ring_rs.at[d, k, s]):
                    copy.start()

            @pl.when(needs(d, k, s))
            def _():
                @pl.when(jnp.logical_and(k > 1, needs(d, k - 1, s)))
                def _():
                    chunk_wait(s, d2d_ss.at[d, s])

                for copy in chunk_copies(
                    b, s, partner, d2d_ss.at[d, s], d2d_rs.at[k - 1, s]
                ):
                    copy.start()

    pass_on(0, 1, 0)
    pass_on(1, 1, 0)
    update([(z, s, c) for s in range(subs)], masked=True)

    @pl.when(c == 1)
    def _():
        for s in range(subs):
            chunk_wait(s, own_rs.at[s])
        update([(z, s, 0) for s in range(subs)])

    @pl.loop(1, k_up)
    def _(k):
        @pl.when(k > 1)
        def _():
            pass_on(0, k, 0)
            pass_on(1, k, 0)
            pair(k - 1, 1)

        pass_on(0, k, 1)
        pass_on(1, k, 1)
        pair(k, 0)

        @pl.when(k == 3)
        def _():
            wout_gather.relay()

        @pl.when(k == 5)
        def _():
            wout_gather.relay_near()
            wout_gather.relay_far()

    for s in range(subs):
        pass_on(s, k_up, s)
    pair(k_up - 1, 1)

    few = rows_tp // 2
    head = NY * x + y

    def send_attended(tile):
        per_tile = QT // rows_tp
        for n in range(tile * per_tile, (tile + 1) * per_tile):
            first = o_s[pl.ds(n * rows_tp, few), :]
            second = o_s[pl.ds(n * rows_tp + few, few), :]
            first = pltpu.roll(first, HEAD, 1) / first
            second = second / pltpu.roll(second, HEAD, 1)
            att_send[n] = jnp.where(low[:few], first, second).astype(BF16)
        for place in (2 * tile, 2 * tile + 1):
            for n in range(2 * NC):
                odd_y, core = n // NC, n % NC
                ty = 2 * c + odd_y
                t = lax.rem(x + place, NX) * NC + core
                piece = (place // 2) * NX * NC + odd_y * NX + (place % 2) * NC + core
                src = att_send.at[piece]
                remote = pltpu.make_async_remote_copy(
                    src_ref=src,
                    dst_ref=att_recv.at[head],
                    send_sem=att_ss,
                    recv_sem=att_rs.at[x],
                    device_id=(z * NY + ty, t),
                    device_id_type=MESH,
                )
                local = pltpu.make_async_copy(src, att_recv.at[head], att_rs.at[x])
                is_self = jnp.logical_and(ty == y, tp == t)

                @pl.when(jnp.logical_not(is_self))
                def _():
                    remote.start()

                @pl.when(is_self)
                def _():
                    local.start()

    @pl.when(z >= k_up)
    def _():
        for s in range(subs):
            chunk_wait(s, d2d_rs.at[k_up - 1, s])
        last = [(z - k_up, s, core) for s in range(subs) for core in range(2)]
        update(last, order=(1, 0), between=lambda: send_attended(1))

    @pl.when(z < k_up)
    def _():
        send_attended(1)

    send_attended(0)

    tok_gather.drain()
    for i in range(2):

        @pl.when(2 * c + i != y)
        def _():
            for n, sent in enumerate((kv_send.at[i], q_send.at[i], gate_send.at[i])):
                pltpu.make_async_copy(sent, sent, a2a_ss.at[n, i]).wait()

    @pl.when(c == 0)
    def _():
        for s in range(subs):
            chunk_wait(s, own_ss.at[s])

    @pl.loop(1, k_up + 1)
    def _(k):
        for d in range(2):
            for s in range(subs):
                more = jnp.logical_not(sends(d, k + 1, s))

                @pl.when(jnp.logical_and(sends(d, k, s), more))
                def _():
                    chunk_wait(s, ring_ss.at[d, s])

                more = jnp.logical_not(needs(d, k + 1, s))

                @pl.when(jnp.logical_and(needs(d, k, s), more))
                def _():
                    chunk_wait(s, d2d_ss.at[d, s])

    wout_gather.finish_own()
    wout_gather.finish_right()
    wout_gather.finish_left()
    wout_gather.finish_far()
    cols = 256
    for n, dx in enumerate((0, 1, -1, 2)):
        slot = lax.rem(x + dx + NX, NX)
        heads = att_recv.at[pl.ds(slot * NY, NY)]
        pltpu.make_async_copy(heads, heads, att_rs.at[slot]).wait()
        pairs = []
        for g in range(NC):
            even, odd = [att_recv[slot * NY + 2 * g + i].astype(F32) for i in range(2)]
            early = jnp.where(low[:few], even, pltpu.roll(odd, HEAD, 1))
            late = jnp.where(low[:few], pltpu.roll(even, HEAD, 1), odd)
            pairs.append(jnp.concatenate([early, late], axis=0).astype(BF16))

        for t in range(out_ref.shape[1] // cols):
            span = pl.ds(t * cols, cols)
            acc = None if n == 0 else acc_s[:, span]
            for g in range(NC):
                first = pl.multiple_of((slot * NC + g) * wout_rows, wout_rows)
                part = jnp.dot(
                    pairs[g], wout[pl.ds(first, wout_rows), span], preferred_element_type=F32
                )
                part = part.astype(BF16).astype(F32)
                acc = part if acc is None else acc + part
            if n < NX - 1:
                acc_s[:, span] = acc
            else:
                out_ref[:, span] = acc.astype(BF16)

    wout_gather.drain()
    stays = owner_core == c
    pieces = att_send.shape[0]

    @pl.when(stays)
    def _():
        sent = att_send.at[pl.ds(0, pieces - 1)]
        pltpu.make_async_copy(sent, sent, att_ss).wait()

    @pl.when(jnp.logical_not(stays))
    def _():
        pltpu.make_async_copy(att_send, att_send, att_ss).wait()


def on_device(
    nz,
    tokens,
    query_weight,
    key_weight,
    value_weight,
    query_gain,
    key_gain,
    log_gate_total,
    output_weight,
):
    rows_tp, depth = tokens.shape
    width = query_weight.shape[1]
    blk, heads = log_gate_total.shape
    half = 2 * blk
    k_up = nz // 2
    dma = pltpu.SemaphoreType.DMA
    any_spec = pl.BlockSpec(memory_space=pl.ANY)
    vmem_spec = pl.BlockSpec(memory_space=pltpu.VMEM)
    return pl.pallas_call(
        functools.partial(kernel, nz),
        out_shape=pltpu.VMEM((rows_tp, output_weight.shape[1]), BF16),
        in_specs=[any_spec] * 8,
        out_specs=vmem_spec,
        scratch_shapes=[
            pltpu.VMEM((blk, depth), BF16),
            pltpu.VMEM((depth, 3 * width), BF16),
            pltpu.VMEM((NX * NC * output_weight.shape[0], output_weight.shape[1]), BF16),
            pltpu.VMEM((blk, width), F32),
            pltpu.VMEM((2, blk, LANES), BF16),
            pltpu.VMEM((2, blk // 2, LANES), BF16),
            pltpu.VMEM((2, 1, HEAD), F32),
            pltpu.VMEM((heads, blk), F32),
            pltpu.VMEM((2, 8, LANES), F32),
            pltpu.VMEM((2, blk // 2, LANES), BF16),
            pltpu.VMEM((2, 8, LANES), F32),
            pltpu.VMEM((nz, 2, 2, blk, LANES), BF16),
            pltpu.VMEM((nz, 2, 8, LANES), F32),
            pltpu.VMEM((half, LANES), BF16),
            pltpu.VMEM((half, LANES), F32),
            pltpu.VMEM((half, LANES), F32),
            pltpu.VMEM((half, LANES), F32),
            pltpu.VMEM((2 * half, LANES), BF16),
            pltpu.VMEM((2 * NX * NC, rows_tp // 2, LANES), BF16),
            pltpu.VMEM((NX * NY, rows_tp // 2, LANES), BF16),
            pltpu.VMEM((rows_tp, output_weight.shape[1]), F32),
            dma((8,)),
            dma,
            dma((13,)),
            dma,
            dma((13,)),
            dma((3, 2)),
            dma((4, 2)),
            dma((2, 2)),
            dma((2, k_up, 2)),
            dma((2, 2)),
            dma((k_up, 2)),
            dma((2,)),
            dma((2,)),
            dma,
            dma((NX,)),
        ],
        compiler_params=pltpu.CompilerParams(
            collective_id=0, has_side_effects=True, vmem_limit_bytes=60 * 1024 * 1024
        ),
    )(
        tokens,
        query_weight,
        key_weight,
        value_weight,
        query_gain[None, :],
        key_gain[None, :],
        log_gate_total.T,
        output_weight,
    )


def solution(mesh):
    placed = (
        P(("sp", "tp"), None),
        P(None, "tp"),
        P(None, "tp"),
        P(None, "tp"),
        P(),
        P(),
        P("sp", "tp"),
        P("tp", None),
    )
    nz = mesh.shape["sp"] // NY
    return jax.shard_map(
        functools.partial(on_device, nz),
        mesh=mesh,
        in_specs=placed,
        out_specs=P(("sp", "tp"), None),
        check_vma=False,
    )
```

```python
import functools

import jax
import jax.numpy as jnp
from jax import lax
from jax.experimental import pallas as pl
from jax.experimental.pallas import tpu as pltpu
from jax.sharding import PartitionSpec as P

NORM_EPS = 1e-06
MESH = pl.DeviceIdType.MESH
F32 = jnp.float32
BF16 = jnp.bfloat16
LANES = 128
HEAD = 64
NX = 4
NY = 4
NC = 2
QT = 384


class RowGather:
    def __init__(self, buf, rows, x, c, ids, ssem, rsem):
        self.buf, self.rows, self.x, self.c = buf, rows, x, c
        self.right, self.left, self.partner = ids
        self.ssem, self.rsem = ssem, rsem
        self.half = buf.shape[1] // 2

    def piece(self, dx, core, part):
        slot = lax.rem(self.x + dx + NX, NX) * NC + core
        rows = pl.ds(pl.multiple_of(slot * self.rows, self.rows), self.rows)
        if part is None:
            return self.buf.at[rows]
        return self.buf.at[rows, pl.ds(part * self.half, self.half)]

    def copy(self, dx, core, part, index):
        device = self.right if index < 3 else self.left if index < 6 else self.partner
        piece = self.piece(dx, core, part)
        return pltpu.make_async_remote_copy(
            src_ref=piece,
            dst_ref=piece,
            send_sem=self.ssem,
            recv_sem=self.rsem.at[index],
            device_id=device,
            device_id_type=MESH,
        )

    def send(self, dx, part, index):
        self.copy(dx, self.c, part, index).start()

    def arrive(self, dx, core, part, index):
        self.copy(dx, core, part, index).wait_recv()

    def start(self):
        self.send(0, 0, 0)
        self.send(0, 1, 3)
        self.send(0, 1, 1)
        self.send(0, 0, 4)
        self.send(0, None, 6)

    def relay(self):
        self.arrive(-1, self.c, 0, 0)
        self.send(-1, 0, 2)
        self.arrive(1, self.c, 1, 3)
        self.send(1, 1, 5)
        self.send(-1, 0, 7)
        self.send(1, 1, 8)

    def relay_near(self):
        self.arrive(1, self.c, 0, 4)
        self.send(1, 0, 10)
        self.arrive(-1, self.c, 1, 1)
        self.send(-1, 1, 9)

    def relay_far(self):
        self.arrive(-2, self.c, 0, 2)
        self.send(-2, 0, 11)
        self.arrive(2, self.c, 1, 5)
        self.send(2, 1, 12)

    def finish_own(self):
        self.arrive(0, 1 - self.c, None, 6)

    def finish_right(self):
        other = 1 - self.c
        self.arrive(1, other, 1, 8)
        self.arrive(1, other, 0, 10)

    def finish_left(self):
        other = 1 - self.c
        self.arrive(-1, other, 0, 7)
        self.arrive(-1, other, 1, 9)

    def finish_far(self):
        other = 1 - self.c
        self.arrive(-2, other, 0, 11)
        self.arrive(2, other, 1, 12)

    def drain(self):
        sent = self.buf.at[pl.ds(0, 7 * self.rows)]
        pltpu.make_async_copy(sent, sent, self.ssem).wait()


def kernel(
    nz,
    tokens_ref,
    wq_ref,
    wk_ref,
    wv_ref,
    qgain_ref,
    kgain_ref,
    gates_ref,
    wout_ref,
    out_ref,
    tok,
    wqkv,
    wout,
    q_raw,
    kv_send,
    q_send,
    gain_v,
    gate_v,
    gate_send,
    q_recv,
    gate_recv,
    kv_all,
    gate_all,
    q_s,
    gt_s,
    m_s,
    o_s,
    v_s,
    k_s,
    att_send,
    att_recv,
    acc_s,
    lsem,
    tok_ss,
    tok_rs,
    wo_ss,
    wo_rs,
    a2a_ss,
    a2a_rs,
    ring_ss,
    ring_rs,
    d2d_ss,
    d2d_rs,
    own_ss,
    own_rs,
    att_ss,
    att_rs,
):
    sp = lax.axis_index("sp")
    tp = lax.axis_index("tp")
    z, y = lax.div(sp, NY), lax.rem(sp, NY)
    x, c = lax.div(tp, NC), lax.rem(tp, NC)

    def device(dz, dy, dx, dc):
        return (dz * NY + dy, dx * NC + dc)

    right = device(z, y, lax.rem(x + 1, NX), c)
    left = device(z, y, lax.rem(x + NX - 1, NX), c)
    partner = device(z, y, x, 1 - c)
    up = device(lax.rem(z + 1, nz), y, x, c)
    down = device(lax.rem(z + nz - 1, nz), y, x, c)
    owner_core = lax.div(y, 2)

    rows_tp = tokens_ref.shape[0]
    blk = rows_tp * NX * NC
    half = 2 * blk
    width = wq_ref.shape[1]

    own_rows = pl.ds(pl.multiple_of(tp * rows_tp, rows_tp), rows_tp)
    wout_rows = wout_ref.shape[0]
    load_tok = pltpu.make_async_copy(tokens_ref, tok.at[own_rows], lsem.at[0])
    load_tok.start()
    loads = []
    for i, w_ref in enumerate((wq_ref, wk_ref, wv_ref)):
        loads.append(
            pltpu.make_async_copy(w_ref, wqkv.at[:, pl.ds(i * width, width)], lsem.at[1 + i])
        )
    load_wout = pltpu.make_async_copy(
        wout_ref,
        wout.at[pl.ds(pl.multiple_of(tp * wout_rows, wout_rows), wout_rows)],
        lsem.at[4],
    )
    for load in loads:
        load.start()
    load_wout.start()
    smalls = []
    for i, (src, dst) in enumerate(
        ((qgain_ref, gain_v.at[0]), (kgain_ref, gain_v.at[1]), (gates_ref, gate_v))
    ):
        smalls.append(pltpu.make_async_copy(src, dst, lsem.at[5 + i]))
        smalls[-1].start()

    barrier = pltpu.get_barrier_semaphore()
    for neighbour in (right, left, partner, up, down):
        pl.semaphore_signal(barrier, inc=1, device_id=neighbour, device_id_type=MESH)
    for i in range(2):
        j = 2 * c + i

        @pl.when(j != y)
        def _():
            pl.semaphore_signal(
                barrier, inc=1, device_id=device(z, j, x, owner_core), device_id_type=MESH
            )

    @pl.when(owner_core == c)
    def _():
        pl.semaphore_wait(barrier, 6)

    @pl.when(owner_core != c)
    def _():
        pl.semaphore_wait(barrier, 7)

    load_tok.wait()
    tok_gather = RowGather(tok, rows_tp, x, c, (right, left, partner), tok_ss, tok_rs)
    tok_gather.start()
    par = lax.rem(y, 2)
    tiles_blk = blk // LANES

    chip_rows = NC * rows_tp
    part_rows = blk // 2
    for small in smalls:
        small.wait()
    sublane = lax.broadcasted_iota(jnp.int32, (8, LANES), 0)
    wide_lane = lax.broadcasted_iota(jnp.int32, (8, half), 1)
    for i in range(2):
        line = jnp.broadcast_to(gate_v[i : i + 1, :], (8, blk))
        turned = line
        for n in range(1, NX):
            turned = jnp.where(x == n, pltpu.roll(line, blk - n * chip_rows, 1), turned)
        line = jnp.concatenate([turned, jnp.zeros((8, half - blk), F32)], axis=1)
        moved = pltpu.roll(line, part_rows, 1)
        first = jnp.where(wide_lane < part_rows, line, 0.0)
        second = jnp.where(wide_lane >= blk, moved, 0.0)
        line = first + second
        line = jnp.where(par == 0, line, pltpu.roll(line, part_rows, 1))
        tile = jnp.zeros((8, LANES), F32)
        for t in range(2 * tiles_blk):
            tile = jnp.where(sublane == t, line[:, t * LANES : (t + 1) * LANES], tile)
        gate_send[i] = tile

    def exchange(n, kind, i, src, dst):
        j = 2 * c + i
        remote = pltpu.make_async_remote_copy(
            src_ref=src,
            dst_ref=dst,
            send_sem=a2a_ss.at[kind, i],
            recv_sem=a2a_rs.at[n, par],
            device_id=device(z, j, x, owner_core),
            device_id_type=MESH,
        )

        @pl.when(j != y)
        def _():
            remote.start()

        @pl.when(j == y)
        def _():
            pltpu.make_async_copy(src, dst, a2a_rs.at[n, par]).start()

    def received(n, s, dst):
        pltpu.make_async_copy(dst, dst, a2a_rs.at[n, s]).wait()

    for i in range(2):
        exchange(3, 2, i, gate_send.at[i], gate_recv.at[par])

    lane = lax.broadcasted_iota(jnp.int32, (LANES, LANES), 1)
    low = lane < HEAD
    qgain, kgain = [jnp.concatenate([gain_v[i], gain_v[i]], axis=1) for i in range(2)]
    def head_norm(raw_part, gain):
        low_part = low[: raw_part.shape[0]]
        square = raw_part * raw_part
        lo = jnp.sum(jnp.where(low_part, square, 0.0), axis=1, keepdims=True) * (1.0 / HEAD)
        hi = jnp.sum(jnp.where(low_part, 0.0, square), axis=1, keepdims=True) * (1.0 / HEAD)
        inverse = jnp.where(low_part, lax.rsqrt(lo + NORM_EPS), lax.rsqrt(hi + NORM_EPS))
        return raw_part * inverse * gain

    def rows_of(dx):
        slot = lax.rem(x + dx + NX, NX)
        return pl.ds(pl.multiple_of(slot * chip_rows, chip_rows), chip_rows)

    def project_keys(dx):
        place = dx % NX
        kept = pl.ds(place * chip_rows, chip_rows)
        low_part = low[:chip_rows]
        raw = jnp.dot(tok[rows_of(dx), :], wqkv[:, width : 3 * width], preferred_element_type=F32)
        k_part = head_norm(raw[:, 0:width], kgain)
        v_part = raw[:, width : 2 * width]
        k_roll = pltpu.roll(k_part, HEAD, 1)
        v_roll = pltpu.roll(v_part, HEAD, 1)
        kv_send[0, kept, :] = jnp.where(low_part, k_part, v_roll).astype(BF16)
        kv_send[1, kept, :] = jnp.where(low_part, k_roll, v_part).astype(BF16)
        chunk = place // 2
        first = pl.multiple_of(par * part_rows + (place % 2) * chip_rows, chip_rows)
        there = kv_all.at[z, chunk, owner_core, pl.ds(first, chip_rows)]
        for i in range(2):
            exchange(chunk, 0, i, kv_send.at[i, kept], there)

    def project_queries(dx):
        raw = jnp.dot(tok[rows_of(dx), :], wqkv[:, 0:width], preferred_element_type=F32)
        kept = pl.ds((dx % NX) * chip_rows, chip_rows)
        q_raw[kept, :] = head_norm(raw, qgain) * (HEAD**-0.5)

    for load in loads:
        load.wait()
    tok_gather.finish_own()
    project_keys(0)
    tok_gather.relay()
    project_queries(0)
    tok_gather.relay_near()
    tok_gather.finish_right()
    project_keys(1)
    tok_gather.finish_left()
    project_keys(-1)
    tok_gather.relay_far()
    load_wout.wait()
    wout_gather = RowGather(wout, wout_rows, x, c, (right, left, partner), wo_ss, wo_rs)
    wout_gather.start()
    project_queries(1)
    tok_gather.finish_far()
    project_keys(2)

    subs = 2

    def chunk_copies(b, s, target, send_sem, recv_sem):
        pieces = (kv_all.at[b, s, c], gate_all.at[b, c])
        return [
            pltpu.make_async_remote_copy(
                src_ref=piece,
                dst_ref=piece,
                send_sem=send_sem,
                recv_sem=recv_sem,
                device_id=target,
                device_id_type=MESH,
            )
            for piece in (pieces if s == 0 else pieces[:1])
        ]

    def chunk_wait(s, sem, count=1):
        gate_rows = 8 * LANES * 4 // (LANES * 2)
        sized = v_s.at[pl.ds(0, count * (blk + gate_rows if s == 0 else blk))]
        pltpu.make_async_copy(sized, sized, sem).wait()

    k_up = nz // 2
    links = (up, down)

    def block_of(d, k):
        return z - k if d == 0 else lax.rem(z + k, nz)

    def whole(d, k, s):
        return k <= (k_up if s == d else k_up - 1)

    def highest(s):
        return k_up - 1 if s == 1 else k_up - 2

    def receives(d, k, s):
        block = block_of(d, k)
        return jnp.logical_and(block >= 0 if d == 0 else block <= highest(s), whole(d, k, s))

    def sends(d, k, s):
        if d == 0:
            there = jnp.logical_and(z - k + 1 >= 0, z <= nz - 2)
        else:
            there = lax.rem(z + k - 1, nz) <= highest(s)
        return jnp.logical_and(there, whole(d, k, s))

    def needs(d, k, s):
        if d == 0:
            return receives(0, k, s)
        return jnp.logical_and(receives(1, k, s), block_of(1, k) < z)

    for s in range(subs):
        received(3, s, gate_recv.at[s])
    gate_all[z, c] = gate_recv[0] + gate_recv[1]
    def own_to_ring(s):
        for n in range(2):
            received(s, n, kv_all.at[z, s, c, pl.ds(n * part_rows, part_rows)])
        for d in range(2):

            @pl.when(sends(d, 1, s))
            def _():
                for copy in chunk_copies(z, s, links[d], ring_ss.at[d, s], ring_rs.at[d, 0, s]):
                    copy.start()

    own_to_ring(0)

    project_queries(-1)
    project_queries(2)
    pack = blk // 2
    step = 64
    for t in range(pack // step):
        first = q_raw[pl.ds(t * step, step), :]
        second = q_raw[pl.ds(pack + t * step, step), :]
        rows = pl.ds(t * step, step)
        q_send[0, rows, :] = jnp.where(low[:step], first, pltpu.roll(second, HEAD, 1)).astype(BF16)
        q_send[1, rows, :] = jnp.where(low[:step], pltpu.roll(first, HEAD, 1), second).astype(BF16)
    for i in range(2):
        exchange(2, 1, i, q_send.at[i], q_recv.at[par])

    own_to_ring(1)

    @pl.when(c == 0)
    def _():
        for s in range(subs):
            for copy in chunk_copies(z, s, partner, own_ss.at[s], own_rs.at[s]):
                copy.start()

    gate_t = jnp.transpose(gate_all[z, c])
    for t in range(2 * tiles_blk):
        column = gate_t[:, t : t + 1]
        gt_s[pl.ds(t * LANES, LANES), :] = jnp.broadcast_to(column, (LANES, LANES))
    m_s[...] = jnp.full(m_s.shape, -1e30, F32)
    o_s[...] = jnp.zeros(o_s.shape, F32)
    for s in range(subs):
        received(2, s, q_recv.at[s])
        for t in range(pack // step):
            packed = q_recv[s, pl.ds(t * step, step), :].astype(F32)
            second = pltpu.roll(packed, HEAD, 1)
            for n, rows in enumerate((packed, second)):
                first_row = n * blk + s * part_rows + t * step
                q_s[pl.ds(first_row, step), :] = jnp.where(low[:step], rows, 0.0).astype(BF16)

    lane_row = lax.broadcasted_iota(jnp.int32, (1, LANES), 1)
    ones_low = jnp.where(lane_row < HEAD, 1.0, 0.0).astype(BF16)
    keep_high = jnp.where(lane_row < HEAD, 0.0, 1.0).astype(BF16)

    def position(row):
        late = (row >= blk).astype(jnp.int32)
        row = row - late * blk
        odd_y = (row >= part_rows).astype(jnp.int32)
        row = row - odd_y * part_rows
        next_slot = (row >= chip_rows).astype(jnp.int32)
        row = row - next_slot * chip_rows
        slot = lax.bitwise_and(2 * late + next_slot + x, NX - 1)
        return odd_y * blk + slot * chip_rows + row

    def update(pieces, masked=False, order=tuple(range(half // QT)), between=None):
        count = len(pieces) * blk

        joined = jnp.concatenate([kv_all[b, s, core] for b, s, core in pieces], axis=0)
        v_s[pl.ds(0, count), :] = joined * keep_high + ones_low
        k_s[:, pl.ds(0, count)] = jnp.transpose(joined)
        gate_row = jnp.concatenate(
            [
                gate_all[b, core, pl.ds(s * tiles_blk + i, 1), :]
                for b, s, core in pieces
                for i in range(tiles_blk)
            ],
            axis=1,
        )

        def score_of(t):
            score = jnp.dot(
                q_s[pl.ds(t * QT, QT), 0:HEAD],
                k_s[0:HEAD, pl.ds(0, count)],
                preferred_element_type=F32,
            )
            score = score - gate_row
            if masked:
                query_pos = position(lax.broadcasted_iota(jnp.int32, (QT, 1), 0) + t * QT)
                key_pos = position(lax.broadcasted_iota(jnp.int32, (1, count), 1))
                score = jnp.where(key_pos <= query_pos, score, -jnp.inf)
            return score

        def add(t, score):
            rows = pl.ds(t * QT, QT)
            gt = gt_s[rows, :]
            m_old = m_s[rows, :]
            m_new = jnp.maximum(m_old, jnp.max(score, axis=1, keepdims=True) + gt)
            wide = jnp.concatenate([m_new - gt] * (count // LANES), axis=1)
            probs = jnp.exp(score - wide).astype(BF16)
            o_s[rows, :] = o_s[rows, :] * jnp.exp(m_old - m_new) + jnp.dot(
                probs, v_s[pl.ds(0, count), :], preferred_element_type=F32
            )
            m_s[rows, :] = m_new

        score = score_of(order[0])
        for n, t in enumerate(order):
            following = score_of(order[n + 1]) if n + 1 < len(order) else None
            add(t, score)
            score = following
            if n == 0 and between is not None:
                between()

    def pieces_of(d, k, s):
        return [(block_of(d, k), s, core) for core in range(2)]

    def pair(k, s):
        @pl.when(needs(1, k, s))
        def _():
            chunk_wait(s, d2d_rs.at[k - 1, s], 2)
            update(pieces_of(0, k, s) + pieces_of(1, k, s))

        @pl.when(jnp.logical_and(needs(0, k, s), jnp.logical_not(needs(1, k, s))))
        def _():
            chunk_wait(s, d2d_rs.at[k - 1, s])
            update(pieces_of(0, k, s))

    def pass_on(d, k, s):
        @pl.when(receives(d, k, s))
        def _():
            b = block_of(d, k)
            chunk_wait(s, ring_rs.at[d, k - 1, s])

            @pl.when(sends(d, k + 1, s))
            def _():
                @pl.when(sends(d, k, s))
                def _():
                    chunk_wait(s, ring_ss.at[d, s])

                for copy in chunk_copies(b, s, links[d], ring_ss.at[d, s], ring_rs.at[d, k, s]):
                    copy.start()

            @pl.when(needs(d, k, s))
            def _():
                @pl.when(jnp.logical_and(k > 1, needs(d, k - 1, s)))
                def _():
                    chunk_wait(s, d2d_ss.at[d, s])

                for copy in chunk_copies(
                    b, s, partner, d2d_ss.at[d, s], d2d_rs.at[k - 1, s]
                ):
                    copy.start()

    pass_on(0, 1, 0)
    pass_on(1, 1, 0)
    update([(z, s, c) for s in range(subs)], masked=True)

    @pl.when(c == 1)
    def _():
        for s in range(subs):
            chunk_wait(s, own_rs.at[s])
        update([(z, s, 0) for s in range(subs)])

    @pl.loop(1, k_up)
    def _(k):
        @pl.when(k > 1)
        def _():
            pass_on(0, k, 0)
            pass_on(1, k, 0)
            pair(k - 1, 1)

        pass_on(0, k, 1)
        pass_on(1, k, 1)
        pair(k, 0)

        @pl.when(k == 3)
        def _():
            wout_gather.relay()

        @pl.when(k == 5)
        def _():
            wout_gather.relay_near()
            wout_gather.relay_far()

    for s in range(subs):
        pass_on(s, k_up, s)
    pair(k_up - 1, 1)

    few = rows_tp // 2
    head = NY * x + y

    def send_attended(tile):
        per_tile = QT // rows_tp
        for n in range(tile * per_tile, (tile + 1) * per_tile):
            first = o_s[pl.ds(n * rows_tp, few), :]
            second = o_s[pl.ds(n * rows_tp + few, few), :]
            first = pltpu.roll(first, HEAD, 1) / first
            second = second / pltpu.roll(second, HEAD, 1)
            att_send[n] = jnp.where(low[:few], first, second).astype(BF16)
        for place in (2 * tile, 2 * tile + 1):
            for n in range(2 * NC):
                odd_y, core = n // NC, n % NC
                ty = 2 * c + odd_y
                t = lax.rem(x + place, NX) * NC + core
                piece = (place // 2) * NX * NC + odd_y * NX + (place % 2) * NC + core
                src = att_send.at[piece]
                remote = pltpu.make_async_remote_copy(
                    src_ref=src,
                    dst_ref=att_recv.at[head],
                    send_sem=att_ss,
                    recv_sem=att_rs.at[x],
                    device_id=(z * NY + ty, t),
                    device_id_type=MESH,
                )
                local = pltpu.make_async_copy(src, att_recv.at[head], att_rs.at[x])
                is_self = jnp.logical_and(ty == y, tp == t)

                @pl.when(jnp.logical_not(is_self))
                def _():
                    remote.start()

                @pl.when(is_self)
                def _():
                    local.start()

    @pl.when(z >= k_up)
    def _():
        for s in range(subs):
            chunk_wait(s, d2d_rs.at[k_up - 1, s])
        last = [(z - k_up, s, core) for s in range(subs) for core in range(2)]
        update(last, order=(1, 0), between=lambda: send_attended(1))

    @pl.when(z < k_up)
    def _():
        send_attended(1)

    send_attended(0)

    tok_gather.drain()
    for i in range(2):

        @pl.when(2 * c + i != y)
        def _():
            for n, sent in enumerate((kv_send.at[i], q_send.at[i], gate_send.at[i])):
                pltpu.make_async_copy(sent, sent, a2a_ss.at[n, i]).wait()

    @pl.when(c == 0)
    def _():
        for s in range(subs):
            chunk_wait(s, own_ss.at[s])

    @pl.loop(1, k_up + 1)
    def _(k):
        for d in range(2):
            for s in range(subs):
                more = jnp.logical_not(sends(d, k + 1, s))

                @pl.when(jnp.logical_and(sends(d, k, s), more))
                def _():
                    chunk_wait(s, ring_ss.at[d, s])

                more = jnp.logical_not(needs(d, k + 1, s))

                @pl.when(jnp.logical_and(needs(d, k, s), more))
                def _():
                    chunk_wait(s, d2d_ss.at[d, s])

    wout_gather.finish_own()
    wout_gather.finish_right()
    wout_gather.finish_left()
    wout_gather.finish_far()
    cols = 256
    for n, dx in enumerate((0, 1, -1, 2)):
        slot = lax.rem(x + dx + NX, NX)
        heads = att_recv.at[pl.ds(slot * NY, NY)]
        pltpu.make_async_copy(heads, heads, att_rs.at[slot]).wait()
        pairs = []
        for g in range(NC):
            even, odd = [att_recv[slot * NY + 2 * g + i].astype(F32) for i in range(2)]
            early = jnp.where(low[:few], even, pltpu.roll(odd, HEAD, 1))
            late = jnp.where(low[:few], pltpu.roll(even, HEAD, 1), odd)
            pairs.append(jnp.concatenate([early, late], axis=0).astype(BF16))

        for t in range(out_ref.shape[1] // cols):
            span = pl.ds(t * cols, cols)
            acc = None if n == 0 else acc_s[:, span]
            for g in range(NC):
                first = pl.multiple_of((slot * NC + g) * wout_rows, wout_rows)
                part = jnp.dot(
                    pairs[g], wout[pl.ds(first, wout_rows), span], preferred_element_type=F32
                )
                part = part.astype(BF16).astype(F32)
                acc = part if acc is None else acc + part
            if n < NX - 1:
                acc_s[:, span] = acc
            else:
                out_ref[:, span] = acc.astype(BF16)

    wout_gather.drain()
    stays = owner_core == c
    pieces = att_send.shape[0]

    @pl.when(stays)
    def _():
        sent = att_send.at[pl.ds(0, pieces - 1)]
        pltpu.make_async_copy(sent, sent, att_ss).wait()

    @pl.when(jnp.logical_not(stays))
    def _():
        pltpu.make_async_copy(att_send, att_send, att_ss).wait()


def on_device(
    nz,
    tokens,
    query_weight,
    key_weight,
    value_weight,
    query_gain,
    key_gain,
    log_gate_total,
    output_weight,
):
    rows_tp, depth = tokens.shape
    width = query_weight.shape[1]
    blk, heads = log_gate_total.shape
    half = 2 * blk
    k_up = nz // 2
    dma = pltpu.SemaphoreType.DMA
    any_spec = pl.BlockSpec(memory_space=pl.ANY)
    vmem_spec = pl.BlockSpec(memory_space=pltpu.VMEM)
    return pl.pallas_call(
        functools.partial(kernel, nz),
        out_shape=pltpu.VMEM((rows_tp, output_weight.shape[1]), BF16),
        in_specs=[any_spec] * 8,
        out_specs=vmem_spec,
        scratch_shapes=[
            pltpu.VMEM((blk, depth), BF16),
            pltpu.VMEM((depth, 3 * width), BF16),
            pltpu.VMEM((NX * NC * output_weight.shape[0], output_weight.shape[1]), BF16),
            pltpu.VMEM((blk, width), F32),
            pltpu.VMEM((2, blk, LANES), BF16),
            pltpu.VMEM((2, blk // 2, LANES), BF16),
            pltpu.VMEM((2, 1, HEAD), F32),
            pltpu.VMEM((heads, blk), F32),
            pltpu.VMEM((2, 8, LANES), F32),
            pltpu.VMEM((2, blk // 2, LANES), BF16),
            pltpu.VMEM((2, 8, LANES), F32),
            pltpu.VMEM((nz, 2, 2, blk, LANES), BF16),
            pltpu.VMEM((nz, 2, 8, LANES), F32),
            pltpu.VMEM((half, LANES), BF16),
            pltpu.VMEM((half, LANES), F32),
            pltpu.VMEM((half, LANES), F32),
            pltpu.VMEM((half, LANES), F32),
            pltpu.VMEM((2 * half, LANES), BF16),
            pltpu.VMEM((LANES, 2 * half), BF16),
            pltpu.VMEM((2 * NX * NC, rows_tp // 2, LANES), BF16),
            pltpu.VMEM((NX * NY, rows_tp // 2, LANES), BF16),
            pltpu.VMEM((rows_tp, output_weight.shape[1]), F32),
            dma((8,)),
            dma,
            dma((13,)),
            dma,
            dma((13,)),
            dma((3, 2)),
            dma((4, 2)),
            dma((2, 2)),
            dma((2, k_up, 2)),
            dma((2, 2)),
            dma((k_up, 2)),
            dma((2,)),
            dma((2,)),
            dma,
            dma((NX,)),
        ],
        compiler_params=pltpu.CompilerParams(
            collective_id=0, has_side_effects=True, vmem_limit_bytes=60 * 1024 * 1024
        ),
    )(
        tokens,
        query_weight,
        key_weight,
        value_weight,
        query_gain[None, :],
        key_gain[None, :],
        log_gate_total.T,
        output_weight,
    )


def solution(mesh):
    placed = (
        P(("sp", "tp"), None),
        P(None, "tp"),
        P(None, "tp"),
        P(None, "tp"),
        P(),
        P(),
        P("sp", "tp"),
        P("tp", None),
    )
    nz = mesh.shape["sp"] // NY
    return jax.shard_map(
        functools.partial(on_device, nz),
        mesh=mesh,
        in_specs=placed,
        out_specs=P(("sp", "tp"), None),
        check_vma=False,
    )
```
